128 devices in a mesh: pp: 16 (over z, y), fs: 4 (over x), tp: 2 (over core).
Axes of the slice: x: 4, y: 4, z: 4, core: 2. Of those that a mesh axis runs over, the one named last changes fastest.
Arguments:
- tokens: bfloat16 [16, 8, 128, 2048], P('pp', ('fs', 'tp')), may hold values from -6 to 6
- layer_norm_scale: float32 [16, 2048], P('pp'), may hold values from 0.1 to 1.9
- input_weight: bfloat16 [16, 2048, 1024], P('pp'), may hold values from -0.125 to 0.125
- filter_weight: float32 [16, 4, 1024], P('pp'), may hold values from -3 to 3
- filter_bias: float32 [16, 1024], P('pp'), may hold values from -2 to 2
- recur_gate_weight: bfloat16 [16, 8, 128, 128], P('pp'), may hold values from -0.5 to 0.5
- recur_gate_bias: float32 [16, 1024], P('pp'), may hold values from -4 to 4
- input_gate_weight: bfloat16 [16, 8, 128, 128], P('pp'), may hold values from -0.5 to 0.5
- input_gate_bias: float32 [16, 1024], P('pp'), may hold values from -4 to 4
- decay_setting: float32 [16, 1024], P('pp'), may hold values from -2 to 8
- spike_log_decay: float32 [16, 128], P('pp'), may hold values from -0.7 to 0, as said below
- output_weight: bfloat16 [16, 1024, 2048], P('pp'), may hold values from -0.375 to 0.375
Outputs:
- result: bfloat16 [16, 8, 128, 2048], P('pp', ('fs', 'tp'))
The draws below stay inside these ranges and needn't reach their ends.
Inputs may be any that keep to these rules, and one draw needn't show every extreme that they name: `spike_log_decay`: zero at most positions; at a few positions of each layer drawn from the seed it lies between log(0.5) and log(0.8).
All inputs are finite; a program needn't handle non-finite values.
Results may differ from the reference program's by a relative error of at most 0.023.
Values may be sent and summed in bfloat16 or wider, within the bound.
A program may use at most 64 MiB of HBM per device.

```python
import math
import jax
import jax.numpy as jnp
from jax import lax

D = 2048
RW = 1024
GB = 8
BW = 128
CONV = 4
LEN = 128
SECTIONS = 16
MICRO = 16
SEQS = 8


def draw_spike_log_decay(key, part):
    marks = jax.random.randint(jax.random.fold_in(key, 11), (SECTIONS, LEN), 0, LEN) < 3
    values = jax.random.uniform(jax.random.fold_in(key, 12), (SECTIONS, LEN), jnp.float32, math.log(0.5), math.log(0.8))
    return jnp.where(marks, values, 0.0).astype(jnp.float32)


def draw_decay_setting(key, part):
    fast_share = 0.6
    fast_low = -1.5
    fast_high = 0.5
    picks = jax.random.uniform(jax.random.fold_in(key, 21), (SECTIONS, RW), jnp.float32)
    quick = jax.random.uniform(jax.random.fold_in(key, 22), (SECTIONS, RW), jnp.float32, fast_low, fast_high)
    slow = jax.random.uniform(jax.random.fold_in(key, 23), (SECTIONS, RW), jnp.float32, 6.0, 8.0)
    return jnp.where(picks < fast_share, quick, slow).astype(jnp.float32)


def steps_of(stream_key, dims, split, least, largest):
    loudness = 1.0
    for position, parts in split:
        draws = jax.random.uniform(jax.random.fold_in(jax.random.fold_in(stream_key, 6), position), (parts,), jnp.float32, least / len(split), largest / len(split))
        loudness = loudness * jnp.repeat(jnp.exp(draws), dims[position] // parts).reshape((-1,) + (1,) * (len(dims) - 1 - position))
    return loudness


def bell_draw(stream_key, dims, spread, limit, shards=(), kind=jnp.bfloat16):
    drawn = spread * jax.random.normal(stream_key, dims, jnp.float32)
    if shards:
        drawn = drawn * steps_of(stream_key, dims, shards, -0.22, 0.18)
    return jnp.clip(drawn, -limit, limit).astype(kind)


def setup_inputs(seed: int = 0) -> dict:
    arg_keys = jax.random.split(jax.random.key(seed), 13)
    tokens = bell_draw(arg_keys[0], (MICRO, SEQS, LEN, D), 1.0, 6.0, ((0, 16), (1, 8)))
    layer_norm_scale = jnp.clip(1.0 + 0.18 * jax.random.normal(arg_keys[1], (SECTIONS, D), jnp.float32), 0.1, 1.9)
    input_weight = bell_draw(arg_keys[2], (SECTIONS, D, RW), D ** -0.5, 0.125, ((0, 16),))
    filter_weight = bell_draw(arg_keys[3], (SECTIONS, CONV, RW), CONV ** -0.5, 3.0, ((0, 16),), jnp.float32)
    filter_bias = bell_draw(arg_keys[4], (SECTIONS, RW), 0.3, 2.0, ((0, 16),), jnp.float32)
    recur_gate_weight = bell_draw(arg_keys[5], (SECTIONS, GB, BW, BW), BW ** -0.5, 0.5, ((0, 16),))
    recur_gate_bias = bell_draw(arg_keys[6], (SECTIONS, RW), 1.0, 4.0, ((0, 16),), jnp.float32)
    input_gate_weight = bell_draw(arg_keys[7], (SECTIONS, GB, BW, BW), BW ** -0.5, 0.5, ((0, 16),))
    input_gate_bias = bell_draw(arg_keys[8], (SECTIONS, RW), 1.0, 4.0, ((0, 16),), jnp.float32)
    decay_setting = draw_decay_setting(jax.random.fold_in(arg_keys[12], 71), 0)
    spike_log_decay = draw_spike_log_decay(jax.random.fold_in(arg_keys[12], 71), 0)
    output_weight = bell_draw(arg_keys[11], (SECTIONS, RW, D), (RW // 4) ** -0.5, 0.375, ((0, 16),))
    return {"tokens": tokens, "layer_norm_scale": layer_norm_scale, "input_weight": input_weight, "filter_weight": filter_weight, "filter_bias": filter_bias, "recur_gate_weight": recur_gate_weight, "recur_gate_bias": recur_gate_bias, "input_gate_weight": input_gate_weight, "input_gate_bias": input_gate_bias, "decay_setting": decay_setting, "spike_log_decay": spike_log_decay, "output_weight": output_weight}


def combine_pair(left, right):
    return (left[0] * right[0], right[0] * left[1] + right[1])

def one_layer(hidden, weight_bundle):
    norm_factor, input_projected, filter_kernel_taps, filter_offset, retention_weight, retention_bias, injection_weight, injection_bias, unscaled_decay, decay_spike, output_projected = weight_bundle
    batch = hidden.shape[0]
    width = input_projected.shape[1]
    taps = filter_kernel_taps.shape[0]
    blocks = retention_weight.shape[0]
    hidden32 = hidden.astype(jnp.float32)
    squares = lax.optimization_barrier(jnp.mean(hidden32 * hidden32, axis=-1, keepdims=True))
    normed = (hidden32 * lax.rsqrt(squares + 1e-06) * norm_factor).astype(jnp.bfloat16)
    mixed_in = jnp.dot(normed.reshape(-1, normed.shape[-1]), input_projected, preferred_element_type=jnp.float32)
    mixed_in = mixed_in.astype(jnp.bfloat16).reshape(batch, -1, width)
    length = mixed_in.shape[1]
    padded = jnp.pad(mixed_in.astype(jnp.float32), ((0, 0), (taps - 1, 0), (0, 0)))
    conv_out = filter_offset + sum((padded[:, k:k + length] * filter_kernel_taps[k] for k in range(taps)))
    conv_out = conv_out.astype(jnp.bfloat16)
    grouped = conv_out.astype(jnp.float32).reshape(batch * length, blocks, -1)
    retention_gate = jax.nn.sigmoid(jnp.einsum('ngi,gij->ngj', grouped, retention_weight.astype(jnp.float32)).reshape(batch, length, width) + retention_bias)
    inject = jax.nn.sigmoid(jnp.einsum('ngi,gij->ngj', grouped, injection_weight.astype(jnp.float32)).reshape(batch, length, width) + injection_bias)
    decay_logarithm = -8.0 * retention_gate * jax.nn.softplus(-unscaled_decay) + decay_spike[None, :, None]
    decay = jnp.exp(decay_logarithm)
    update = jnp.sqrt(-jnp.expm1(2.0 * decay_logarithm)) * inject * conv_out.astype(jnp.float32)
    states = lax.associative_scan(combine_pair, (decay, update), axis=1)[1].astype(jnp.bfloat16)
    projected = jnp.dot(states.reshape(-1, width), output_projected, preferred_element_type=jnp.float32)
    return (hidden32 + projected.reshape(hidden.shape)).astype(jnp.bfloat16)

def reference(tokens, layer_norm_scale, input_weight, filter_weight, filter_bias, recur_gate_weight, recur_gate_bias, input_gate_weight, input_gate_bias, decay_setting, spike_log_decay, output_weight):
    hidden = tokens.reshape(-1, tokens.shape[2], tokens.shape[3])

    def advance(carry, weight_bundle):
        return (one_layer(carry, weight_bundle), None)
    layer_stacked_params = (layer_norm_scale, input_weight, filter_weight, filter_bias, recur_gate_weight, recur_gate_bias, input_gate_weight, input_gate_bias, decay_setting, spike_log_decay, output_weight)
    hidden, unused = lax.scan(advance, hidden, layer_stacked_params)
    return hidden.reshape(tokens.shape)
```

```python
import functools

import jax
import jax.numpy as jnp
from jax import lax
from jax.experimental import pallas as pl
from jax.experimental.pallas import tpu as pltpu
from jax.sharding import PartitionSpec as P

PLANE = 4
SUB = 8
PARTS = 16
MESH = pl.DeviceIdType.MESH


def shifted(blocks, masked, delay):
    steps = blocks.shape[0]
    if delay == 0:
        return blocks
    return jnp.concatenate([masked[3 - delay :], blocks[: steps - delay]], axis=0)


def layer(hidden, win, wout, gates, vec, spike, normed, states):
    length, width = hidden.shape
    inner = win.shape[1]
    steps = length // SUB
    top = lax.broadcasted_iota(jnp.int32, (SUB, 128), 0)

    total = jnp.zeros((length, 128), jnp.float32)
    for n in range(width // 128):
        part = hidden[:, n * 128 : (n + 1) * 128].astype(jnp.float32)
        total = total + part * part
    scale = lax.rsqrt(jnp.sum(total, axis=1, keepdims=True) * (1.0 / width) + 1e-6)
    for n in range(width // 256):
        cols = slice(n * 256, (n + 1) * 256)
        row, start = divmod(n * 256, inner)
        gain = vec[row : row + 1, start : start + 256]
        normed[:, cols] = (hidden[:, cols].astype(jnp.float32) * scale * gain).astype(jnp.bfloat16)

    spikes = spike[...].reshape(steps, SUB, 128)
    for n in range(inner // 256):
        mixed2 = jnp.dot(
            normed[...], win[:, n * 256 : (n + 1) * 256], preferred_element_type=jnp.float32
        )
        for half in range(2):
            block = 2 * n + half
            cols = slice(block * 128, (block + 1) * 128)
            mixed = mixed2[:, half * 128 : (half + 1) * 128]
            mixed = mixed.astype(jnp.bfloat16).astype(jnp.float32).reshape(steps, SUB, 128)
            before = [
                jnp.where(top == 0, 0.0, pltpu.roll(mixed[steps - 3 + d], 1, 0))[None]
                for d in range(3)
            ]
            before = jnp.concatenate(before, axis=0)
            conv = vec[6:7, cols][None] + sum(
                shifted(mixed, before, 3 - k) * vec[2 + k : 3 + k, cols][None] for k in range(4)
            )
            conv = conv.reshape(length, 128).astype(jnp.bfloat16)
            pre = jnp.dot(
                conv, gates[block * 128 : (block + 1) * 128, :], preferred_element_type=jnp.float32
            )
            recall = 0.5 * jnp.tanh(0.5 * (pre[:, :128] + vec[7:8, cols])) + 0.5
            inject = 0.5 * jnp.tanh(0.5 * (pre[:, 128:] + vec[8:9, cols])) + 0.5
            log_decay = recall.reshape(steps, SUB, 128) * vec[9:10, cols][None] + spikes
            decay = jnp.exp(log_decay)
            update = (
                jnp.sqrt(jnp.maximum(1.0 - decay * decay, 0.0))
                * inject.reshape(steps, SUB, 128)
                * conv.astype(jnp.float32).reshape(steps, SUB, 128)
            )
            sums = [update[0]]
            factors = [decay[0]]
            for t in range(1, steps):
                sums.append(decay[t] * sums[-1] + update[t])
                factors.append(decay[t] * factors[-1])
            last, factor = sums[-1], factors[-1]
            for hop in (1, 2, 4):
                last = last + factor * jnp.where(top < hop, 0.0, pltpu.roll(last, hop, 0))
                if hop < 4:
                    factor = factor * jnp.where(top < hop, 1.0, pltpu.roll(factor, hop, 0))
            carry = jnp.where(top == 0, 0.0, pltpu.roll(last, 1, 0))
            done = jnp.concatenate(
                [(sums[t] + factors[t] * carry)[None] for t in range(steps)], axis=0
            )
            states[:, cols] = done.reshape(length, 128).astype(jnp.bfloat16)

    for n in range(width // 256):
        cols = slice(n * 256, (n + 1) * 256)
        projected = jnp.dot(states[...], wout[:, cols], preferred_element_type=jnp.float32)
        hidden[:, cols] = (hidden[:, cols].astype(jnp.float32) + projected).astype(jnp.bfloat16)


def kernel(
    planes, columns,
    tok, win, wout, gates, vec, spike, out,
    win_all, wout_all, gates_all, vec_all, spike_all, act, normed, states,
    y_recv, x_recv, d_recv, y_send, x_send, d_send, own_sem,
    small_recv, small_send, act_recv, act_send, tok_sem, out_recv,
):
    position = lax.axis_index("pp")
    x = lax.axis_index("fs")
    core = lax.axis_index("tp")
    z = position // PLANE
    y = lax.rem(position, PLANE)
    parity = lax.rem(x, 2)

    def at_y(by):
        return z * PLANE + lax.rem(y + by, PLANE)

    def plane_slot(by):
        return lax.rem(y + by, PLANE)

    up, down, across = {"pp": at_y(1)}, {"pp": at_y(3)}, {"pp": at_y(2)}
    right, left = {"fs": lax.rem(x + 1, columns)}, {"fs": lax.rem(x + columns - 1, columns)}
    sibling = {"tp": 1 - core}
    z_peers = [{"pp": lax.rem(z + by, planes) * PLANE + y} for by in range(1, planes)]

    barrier = pltpu.get_barrier_semaphore()
    peers = [up, down, across, right, left, sibling] + z_peers
    for peer in peers:
        pl.semaphore_signal(barrier, inc=1, device_id=peer, device_id_type=MESH)
    pl.semaphore_wait(barrier, len(peers))

    sources = (win, wout, gates)
    gathered = (win_all, wout_all, gates_all)
    heights = tuple(ref.shape[0] // PARTS for ref in sources)

    def piece_rows(a, piece):
        return pl.ds(pl.multiple_of(piece * heights[a], heights[a]), heights[a])

    def send(a, src, slot, piece, send_sem, recv_sem, to):
        pltpu.make_async_remote_copy(
            src_ref=src,
            dst_ref=gathered[a].at[slot, piece_rows(a, piece)],
            send_sem=send_sem,
            recv_sem=recv_sem,
            device_id=to,
            device_id_type=MESH,
        ).start()

    def await_bytes(ref, sem):
        pltpu.make_async_copy(ref, ref, sem).wait()

    mine = 8 * parity + 4 * core
    other = 8 * (1 - parity) + 4 * core

    for unit in range(4):
        for a in range(3):
            j = unit
            send(a, sources[a].at[piece_rows(a, mine + j)], y, mine + j,
                 y_send.at[0, a], y_recv.at[0, unit, a], up)
            j = (unit + 2) % 4
            send(a, sources[a].at[piece_rows(a, mine + j)], y, mine + j,
                 y_send.at[1, a], y_recv.at[1, unit, a], down)
    smalls = ((vec, vec_all), (spike, spike_all))
    for n, (src, dst) in enumerate(smalls):
        for by in range(1, 4):
            pltpu.make_async_remote_copy(
                src_ref=src, dst_ref=dst.at[y], send_sem=small_send.at[n, by - 1],
                recv_sem=small_recv.at[n, by - 1],
                device_id={"pp": at_y(by)}, device_id_type=MESH,
            ).start()

    @pl.when(z != 0)
    def _():
        pltpu.make_async_remote_copy(
            src_ref=tok, dst_ref=act.at[z], send_sem=tok_sem, recv_sem=act_recv.at[z],
            device_id={"pp": y}, device_id_type=MESH,
        ).start()

    @pl.when(z == 0)
    def _():
        pltpu.make_async_copy(tok, act.at[0], act_recv.at[0]).start()

    own = [pltpu.make_async_copy(sources[a], gathered[a].at[y], own_sem.at[a]) for a in range(3)]
    own += [pltpu.make_async_copy(src, dst.at[y], own_sem.at[3 + n])
            for n, (src, dst) in enumerate(smalls)]
    for copy in own:
        copy.start()

    def arrivals(unit):
        from_below = (plane_slot(3), unit) if unit < 4 else (plane_slot(2), unit - 4)
        from_above = (plane_slot(1), (unit + 2) % 4) if unit < 4 else (plane_slot(2), unit - 2)
        return from_below, from_above

    def relay_x(unit, a):
        for side, (slot, j) in enumerate(x_units[unit]):
            ref = gathered[a].at[slot, piece_rows(a, other + j)]
            await_bytes(ref, x_recv.at[side, unit, a])
            send(a, ref, slot, other + j, d_send.at[a], d_recv.at[a], sibling)

    x_units = []
    for unit in range(6):
        below, above = arrivals(unit)
        x_units.append((below, above) if below[1] < 2 else (above, below))

    for unit in range(7):
        for a in range(3):
            if unit < 6:
                below, above = arrivals(unit)
                for side, (slot, j) in enumerate((below, above)):
                    ref = gathered[a].at[slot, piece_rows(a, mine + j)]
                    await_bytes(ref, y_recv.at[side, unit, a])
                    if unit < 2:
                        send(a, ref, slot, mine + j, y_send.at[side, a],
                             y_recv.at[side, 4 + unit, a], up if side == 0 else down)
                    x_side = 0 if j < 2 else 1
                    send(a, ref, slot, mine + j, x_send.at[x_side, a],
                         x_recv.at[x_side, unit, a], left if x_side == 0 else right)
                    send(a, ref, slot, mine + j, d_send.at[a], d_recv.at[a], sibling)
            if unit > 0:
                relay_x(unit - 1, a)

    for copy in own:
        copy.wait()
    for n, (src, dst) in enumerate(smalls):
        for by in range(1, 4):
            await_bytes(dst.at[plane_slot(4 - by)], small_recv.at[n, by - 1])
    for a in range(3):
        whole = gathered[a].at[pl.ds(0, 2), pl.ds(0, 12 * heights[a])]
        await_bytes(whole, d_recv.at[a])

    def micro(i, token):
        await_bytes(act.at[i], act_recv.at[i])

        def one(s, token):
            layer(act.at[i], win_all.at[s], wout_all.at[s], gates_all.at[s],
                  vec_all.at[s], spike_all.at[s], normed, states)
            return token

        lax.fori_loop(0, PLANE, one, 0)

        @pl.when(z < planes - 1)
        def _():
            pltpu.make_async_remote_copy(
                src_ref=act.at[i], dst_ref=act.at[i], send_sem=act_send.at[i],
                recv_sem=act_recv.at[i],
                device_id={"pp": lax.rem(z + 1, planes) * PLANE + y}, device_id_type=MESH,
            ).start()

        @pl.when((z == planes - 1) & (i < planes - 1))
        def _():
            pltpu.make_async_remote_copy(
                src_ref=act.at[i], dst_ref=out, send_sem=act_send.at[i],
                recv_sem=out_recv,
                device_id={"pp": i * PLANE + y}, device_id_type=MESH,
            ).start()

        @pl.when((z == planes - 1) & (i == planes - 1))
        def _():
            pltpu.make_async_copy(act.at[i], out, out_recv).start()

        return token

    lax.fori_loop(0, planes, micro, 0)

    await_bytes(out, out_recv)
    for i in range(planes):
        if i < planes - 1:
            await_bytes(act.at[i], act_send.at[i])
        else:
            @pl.when(z < planes - 1)
            def _():
                await_bytes(act.at[i], act_send.at[i])

    @pl.when(z != 0)
    def _():
        await_bytes(tok, tok_sem)

    for n, (src, dst) in enumerate(smalls):
        for by in range(1, 4):
            await_bytes(src, small_send.at[n, by - 1])
    for a in range(3):
        for side in range(2):
            half = gathered[a].at[0, pl.ds(0, 6 * heights[a])]
            await_bytes(half, y_send.at[side, a])
            await_bytes(half, x_send.at[side, a])
        whole = gathered[a].at[pl.ds(0, 2), pl.ds(0, 12 * heights[a])]
        await_bytes(whole, d_send.at[a])


def by_lane(rows):
    length = rows.shape[0]
    return rows.reshape(SUB, length // SUB, -1).swapaxes(0, 1).reshape(length, -1)


def by_time(rows):
    length = rows.shape[0]
    return rows.reshape(length // SUB, SUB, -1).swapaxes(0, 1).reshape(length, -1)


def local(
    tokens,
    layer_norm_scale,
    input_weight,
    filter_weight,
    filter_bias,
    recur_gate_weight,
    recur_gate_bias,
    input_gate_weight,
    input_gate_bias,
    decay_setting,
    spike_log_decay,
    output_weight,
):
    planes = lax.axis_size("pp") // PLANE
    columns = lax.axis_size("fs")
    length, width = tokens.shape[2:]
    inner = input_weight.shape[2]
    tok = by_lane(tokens[0, 0])
    gates = jnp.concatenate([recur_gate_weight[0], input_gate_weight[0]], axis=2).reshape(inner, 256)
    vec = jnp.concatenate(
        [
            layer_norm_scale[0].reshape(-1, inner),
            filter_weight[0],
            filter_bias,
            recur_gate_bias,
            input_gate_bias,
            -8.0 * jax.nn.softplus(-decay_setting),
            jnp.zeros((16 - 8 - width // inner, inner), jnp.float32),
        ],
        axis=0,
    )
    spike = jnp.broadcast_to(by_lane(spike_log_decay[0][:, None]), (length, 128))
    dma = pltpu.SemaphoreType.DMA
    hbm = pl.BlockSpec(memory_space=pl.ANY)
    finished = pl.pallas_call(
        functools.partial(kernel, planes, columns),
        out_shape=jax.ShapeDtypeStruct((length, width), jnp.bfloat16),
        in_specs=[hbm] * 6,
        out_specs=hbm,
        scratch_shapes=[
            pltpu.VMEM((PLANE, width, inner), jnp.bfloat16),
            pltpu.VMEM((PLANE, inner, width), jnp.bfloat16),
            pltpu.VMEM((PLANE, inner, 256), jnp.bfloat16),
            pltpu.VMEM((PLANE, 16, inner), jnp.float32),
            pltpu.VMEM((PLANE, length, 128), jnp.float32),
            pltpu.VMEM((planes, length, width), jnp.bfloat16),
            pltpu.VMEM((length, width), jnp.bfloat16),
            pltpu.VMEM((length, inner), jnp.bfloat16),
            dma((2, 6, 3)),
            dma((2, 6, 3)),
            dma((3,)),
            dma((2, 3)),
            dma((2, 3)),
            dma((3,)),
            dma((5,)),
            dma((2, 3)),
            dma((2, 3)),
            dma((planes,)),
            dma((planes,)),
            dma,
            dma,
        ],
        compiler_params=pltpu.CompilerParams(
            collective_id=0, has_side_effects=True, vmem_limit_bytes=60 * 1024 * 1024
        ),
    )(tok, input_weight[0], output_weight[0], gates, vec, spike)
    return by_time(finished)[None, None]


def solution(mesh):
    placed = (
        P("pp", ("fs", "tp"), None, None),
        P("pp", None),
        P("pp", None, None),
        P("pp", None, None),
        P("pp", None),
        P("pp", None, None, None),
        P("pp", None),
        P("pp", None, None, None),
        P("pp", None),
        P("pp", None),
        P("pp", None),
        P("pp", None, None),
    )
    return jax.shard_map(
        local,
        mesh=mesh,
        in_specs=placed,
        out_specs=P("pp", ("fs", "tp"), None, None),
        check_vma=False,
    )
```

```python
import functools

import jax
import jax.numpy as jnp
from jax import lax
from jax.experimental import pallas as pl
from jax.experimental.pallas import tpu as pltpu
from jax.sharding import PartitionSpec as P

PLANE = 4
SUB = 8
HALVES = 2
PARTS = 16
MESH = pl.DeviceIdType.MESH


def layer(hidden, win, wout, gates, vec, spike, tail, past, scaled, states):
    length, width = hidden.shape
    inner = win.shape[1]
    steps = length // SUB
    top = lax.broadcasted_iota(jnp.int32, (SUB, 128), 0)

    total = jnp.zeros((length, 128), jnp.float32)
    for n in range(width // 128):
        cols = slice(n * 128, (n + 1) * 128)
        row, start = divmod(n * 128, inner)
        part = hidden[:, cols].astype(jnp.float32)
        total = total + part * part
        scaled[:, cols] = (part * vec[row : row + 1, start : start + 128]).astype(jnp.bfloat16)
    scale = lax.rsqrt(jnp.sum(total, axis=1, keepdims=True) * (1.0 / width) + 1e-6)
    scale = jnp.broadcast_to(scale, (length, 128))
    spikes = spike[...].reshape(steps, SUB, 128)

    def project(n):
        return jnp.dot(
            scaled[...], win[:, n * 256 : (n + 1) * 256], preferred_element_type=jnp.float32
        )

    def recur(mixed, block):
        cols = slice(block * 128, (block + 1) * 128)
        mixed = (mixed * scale).astype(jnp.bfloat16).astype(jnp.float32).reshape(steps, SUB, 128)
        taps = [vec[2 + k : 3 + k, cols] for k in range(4)]
        bias = vec[6:7, cols]
        before = []
        for d in range(3):
            rows = slice(d * SUB, (d + 1) * SUB)
            rolled = pltpu.roll(mixed[steps - 3 + d], 1, 0)
            before.append(jnp.where(top == 0, tail[rows, cols], rolled))
            tail[rows, cols] = rolled
        line = before + [mixed[t] for t in range(steps)]
        conv = jnp.concatenate(
            [
                (bias + sum(line[t + k] * taps[k] for k in range(4)))[None]
                for t in range(steps)
            ],
            axis=0,
        )
        conv = conv.reshape(length, 128).astype(jnp.bfloat16)
        pre = jnp.dot(
            conv, gates[block], preferred_element_type=jnp.float32
        )
        recall = 0.5 * jnp.tanh(0.5 * (pre[:, :128] + vec[7:8, cols])) + 0.5
        inject = 0.5 * jnp.tanh(0.5 * (pre[:, 128:] + vec[8:9, cols])) + 0.5
        log_decay = recall.reshape(steps, SUB, 128) * vec[9:10, cols][None] + spikes
        decay = jnp.exp(log_decay)
        room = jnp.maximum(1.0 - decay * decay, 1e-30)
        update = (
            room * lax.rsqrt(room)
            * inject.reshape(steps, SUB, 128)
            * conv.astype(jnp.float32).reshape(steps, SUB, 128)
        )
        sums = [update[0]]
        factors = [decay[0]]
        for t in range(1, steps):
            sums.append(decay[t] * sums[-1] + update[t])
            factors.append(decay[t] * factors[-1])
        first = past[:, cols]
        factor = factors[-1]
        last = sums[-1] + jnp.where(top == 0, factor * first, 0.0)
        for hop in (1, 2, 4):
            last = last + factor * jnp.where(top < hop, 0.0, pltpu.roll(last, hop, 0))
            if hop < 4:
                factor = factor * jnp.where(top < hop, 1.0, pltpu.roll(factor, hop, 0))
        ahead = pltpu.roll(last, 1, 0)
        past[:, cols] = ahead
        carry = jnp.where(top == 0, first, ahead)
        done = jnp.concatenate(
            [(sums[t] + factors[t] * carry)[None] for t in range(steps)], axis=0
        )
        states[:, cols] = done.reshape(length, 128).astype(jnp.bfloat16)

    groups = inner // 256
    mixed = project(0)
    for n in range(groups):
        following = project(n + 1) if n + 1 < groups else None
        recur(mixed[:, :128], 2 * n)
        recur(mixed[:, 128:], 2 * n + 1)
        mixed = following

    for n in range(width // 256):
        cols = slice(n * 256, (n + 1) * 256)
        projected = jnp.dot(states[...], wout[:, cols], preferred_element_type=jnp.float32)
        hidden[:, cols] = (hidden[:, cols].astype(jnp.float32) + projected).astype(jnp.bfloat16)


def reorder(src, dst):
    length = src.shape[0]
    steps = length // SUB
    row = lax.broadcasted_iota(jnp.int32, (length, length), 0)
    col = lax.broadcasted_iota(jnp.int32, (length, length), 1)
    swap = jnp.where(col == lax.rem(row, SUB) * steps + lax.div(row, SUB), 1.0, 0.0)
    swap = swap.astype(jnp.bfloat16)
    for n in range(src.shape[1] // 256):
        cols = slice(n * 256, (n + 1) * 256)
        moved = jnp.dot(swap, src[:, cols], preferred_element_type=jnp.float32)
        dst[:, cols] = moved.astype(jnp.bfloat16)


def kernel(
    planes, columns,
    tok, gain, win, taps, conv_bias, recur_gate, recur_bias, input_gate, input_bias, setting,
    spikes, wout, out,
    win_all, wout_all, gates_all, vec_all, spike_all, raw, home, act, final, tails, pasts,
    scaled, states,
    y_recv, x_recv, d_recv, y_send, x_send, d_send, own_sem,
    small_recv, small_send, raw_sem, act_recv, act_send, home_sem, out_recv,
):
    position = lax.axis_index("pp")
    x = lax.axis_index("fs")
    core = lax.axis_index("tp")
    z = position // PLANE
    y = lax.rem(position, PLANE)
    parity = lax.rem(x, 2)
    length, width = raw.shape
    inner = win_all.shape[2]
    chunk = length // HALVES

    def at_y(by):
        return z * PLANE + lax.rem(y + by, PLANE)

    def plane_slot(by):
        return lax.rem(y + by, PLANE)

    def rows_of(half):
        return pl.ds(pl.multiple_of(half * chunk, chunk), chunk)

    up, down, across = {"pp": at_y(1)}, {"pp": at_y(3)}, {"pp": at_y(2)}
    right, left = {"fs": lax.rem(x + 1, columns)}, {"fs": lax.rem(x + columns - 1, columns)}
    sibling = {"tp": 1 - core}
    z_peers = [{"pp": lax.rem(z + by, planes) * PLANE + y} for by in range(1, planes)]

    own = [
        pltpu.make_async_copy(recur_gate.at[0], gates_all.at[y, :, :, pl.ds(0, 128)], own_sem.at[0]),
        pltpu.make_async_copy(input_gate.at[0], gates_all.at[y, :, :, pl.ds(128, 128)], own_sem.at[1]),
        pltpu.make_async_copy(win.at[0], win_all.at[y], own_sem.at[2]),
        pltpu.make_async_copy(wout.at[0], wout_all.at[y], own_sem.at[3]),
    ]
    for copy in own[:2]:
        copy.start()
    pltpu.make_async_copy(tok.at[0, 0], raw, raw_sem).start()

    barrier = pltpu.get_barrier_semaphore()
    peers = [up, down, across, right, left, sibling] + z_peers
    for peer in peers:
        pl.semaphore_signal(barrier, inc=1, device_id=peer, device_id_type=MESH)

    vec_all[y, 0:1] = gain[:, :inner]
    vec_all[y, 1:2] = gain[:, inner:]
    vec_all[y, 2:6] = taps[0]
    vec_all[y, 6:7] = conv_bias[...]
    vec_all[y, 7:8] = recur_bias[...]
    vec_all[y, 8:9] = input_bias[...]
    below = -setting[...]
    vec_all[y, 9:10] = -8.0 * (jnp.maximum(below, 0.0) + jnp.log1p(jnp.exp(-jnp.abs(below))))
    row = lax.broadcasted_iota(jnp.int32, (length, length), 0)
    col = lax.broadcasted_iota(jnp.int32, (length, length), 1)
    within = lax.rem(row, chunk)
    token = (row - within) + lax.rem(within, SUB) * (chunk // SUB) + lax.div(within, SUB)
    picked = jnp.sum(jnp.where(col == token, spikes[...], 0.0), axis=1, keepdims=True)
    spike_all[y] = jnp.broadcast_to(picked, (length, 128))

    pl.semaphore_wait(barrier, len(peers))

    gathered = (win_all, wout_all, gates_all)

    def piece(ref, a, index):
        if a == 2:
            return ref.at[index // 2, pl.ds(pl.multiple_of(lax.rem(index, 2) * 64, 64), 64)]
        height = win_all.shape[1] // PARTS if a == 0 else wout_all.shape[1] // PARTS
        return ref.at[pl.ds(pl.multiple_of(index * height, height), height)]

    def send(a, src, slot, index, send_sem, recv_sem, to):
        pltpu.make_async_remote_copy(
            src_ref=src,
            dst_ref=piece(gathered[a].at[slot], a, index),
            send_sem=send_sem,
            recv_sem=recv_sem,
            device_id=to,
            device_id_type=MESH,
        ).start()

    def await_bytes(ref, sem):
        pltpu.make_async_copy(ref, ref, sem).wait()

    def pieces_of(a, count):
        if a == 2:
            if count <= PARTS:
                return gates_all.at[0, pl.ds(0, count // 2)]
            return gates_all.at[pl.ds(0, 2), pl.ds(0, count // 4)]
        height = gathered[a].shape[1] // PARTS
        if count <= PARTS:
            return gathered[a].at[0, pl.ds(0, count * height)]
        return gathered[a].at[pl.ds(0, 2), pl.ds(0, count // 2 * height)]

    mine = 8 * parity + 4 * core
    other = 8 * (1 - parity) + 4 * core

    for unit in range(4):
        for a in range(3):
            if unit == 0 and a == 2:
                for copy in own[:2]:
                    copy.wait()
            source = (win.at[0], wout.at[0], gates_all.at[y])[a]
            j = unit
            send(a, piece(source, a, mine + j), y, mine + j,
                 y_send.at[0, a], y_recv.at[0, unit, a], up)
            j = (unit + 2) % 4
            send(a, piece(source, a, mine + j), y, mine + j,
                 y_send.at[1, a], y_recv.at[1, unit, a], down)
    smalls = (vec_all, spike_all)
    for n, ref in enumerate(smalls):
        for by in range(1, 4):
            pltpu.make_async_remote_copy(
                src_ref=ref.at[y], dst_ref=ref.at[y], send_sem=small_send.at[n, by - 1],
                recv_sem=small_recv.at[n, by - 1],
                device_id={"pp": at_y(by)}, device_id_type=MESH,
            ).start()
    for copy in own[2:]:
        copy.start()

    await_bytes(raw, raw_sem)
    for half in range(HALVES):
        rows = slice(half * chunk, (half + 1) * chunk)
        reorder(raw.at[rows], home.at[rows])

        @pl.when(z != 0)
        def _():
            pltpu.make_async_remote_copy(
                src_ref=home.at[rows], dst_ref=act.at[z, rows], send_sem=home_sem.at[half],
                recv_sem=act_recv.at[z, half],
                device_id={"pp": y}, device_id_type=MESH,
            ).start()

        @pl.when(z == 0)
        def _():
            pltpu.make_async_copy(home.at[rows], act.at[0, rows], act_recv.at[0, half]).start()

    def arrivals(unit):
        from_below = (plane_slot(3), unit) if unit < 4 else (plane_slot(2), unit - 4)
        from_above = (plane_slot(1), (unit + 2) % 4) if unit < 4 else (plane_slot(2), unit - 2)
        return from_below, from_above

    x_units = []
    for unit in range(6):
        below, above = arrivals(unit)
        x_units.append((below, above) if below[1] < 2 else (above, below))

    def relay_y(unit, a):
        for side, (slot, j) in enumerate(arrivals(unit)):
            ref = piece(gathered[a].at[slot], a, mine + j)
            await_bytes(ref, y_recv.at[side, unit, a])
            if unit < 2:
                send(a, ref, slot, mine + j, y_send.at[side, a],
                     y_recv.at[side, 4 + unit, a], up if side == 0 else down)
            x_side = 0 if j < 2 else 1
            send(a, ref, slot, mine + j, x_send.at[x_side, a],
                 x_recv.at[x_side, unit, a], left if x_side == 0 else right)
            send(a, ref, slot, mine + j, d_send.at[a], d_recv.at[a], sibling)

    def relay_x(unit, a):
        for side, (slot, j) in enumerate(x_units[unit]):
            ref = piece(gathered[a].at[slot], a, other + j)
            await_bytes(ref, x_recv.at[side, unit, a])
            send(a, ref, slot, other + j, d_send.at[a], d_recv.at[a], sibling)

    for unit in range(7):
        for a in range(3):
            if unit < 6:
                relay_y(unit, a)
            if unit > 0:
                relay_x(unit - 1, a)

    for copy in own[2:]:
        copy.wait()
    for n, ref in enumerate(smalls):
        for by in range(1, 4):
            await_bytes(ref.at[plane_slot(4 - by)], small_recv.at[n, by - 1])
    for a in range(3):
        await_bytes(pieces_of(a, 24), d_recv.at[a])

    def micro(step, token):
        i = step // HALVES
        half = lax.rem(step, HALVES)
        rows = rows_of(half)
        here = act.at[i, rows]
        await_bytes(here, act_recv.at[i, half])

        @pl.when(half == 0)
        def _():
            tails[...] = jnp.zeros_like(tails)
            pasts[...] = jnp.zeros_like(pasts)

        def one(s, token):
            layer(here, win_all.at[s], wout_all.at[s], gates_all.at[s], vec_all.at[s],
                  spike_all.at[s, rows], tails.at[s], pasts.at[s], scaled, states)
            return token

        lax.fori_loop(0, PLANE, one, 0)

        @pl.when(z < planes - 1)
        def _():
            pltpu.make_async_remote_copy(
                src_ref=here, dst_ref=here, send_sem=act_send.at[i, half],
                recv_sem=act_recv.at[i, half],
                device_id={"pp": lax.rem(z + 1, planes) * PLANE + y}, device_id_type=MESH,
            ).start()

        @pl.when(z == planes - 1)
        def _():
            reorder(here, final.at[i, rows])

            @pl.when(i < planes - 1)
            def _():
                pltpu.make_async_remote_copy(
                    src_ref=final.at[i, rows], dst_ref=out.at[0, 0, rows],
                    send_sem=act_send.at[i, half], recv_sem=out_recv.at[half],
                    device_id={"pp": i * PLANE + y}, device_id_type=MESH,
                ).start()

            @pl.when(i == planes - 1)
            def _():
                pltpu.make_async_copy(
                    final.at[i, rows], out.at[0, 0, rows], out_recv.at[half]
                ).start()

        return token

    lax.fori_loop(0, planes * HALVES, micro, 0)

    for half in range(HALVES):
        rows = slice(half * chunk, (half + 1) * chunk)
        await_bytes(out.at[0, 0, rows], out_recv.at[half])
        for i in range(planes):
            if i < planes - 1:
                await_bytes(act.at[i, rows], act_send.at[i, half])
            else:
                @pl.when(z < planes - 1)
                def _():
                    await_bytes(act.at[i, rows], act_send.at[i, half])

        @pl.when(z != 0)
        def _():
            await_bytes(home.at[rows], home_sem.at[half])

    for n, ref in enumerate(smalls):
        for by in range(1, 4):
            await_bytes(ref.at[y], small_send.at[n, by - 1])
    for a in range(3):
        for side in range(2):
            await_bytes(pieces_of(a, 6), y_send.at[side, a])
            await_bytes(pieces_of(a, 6), x_send.at[side, a])
        await_bytes(pieces_of(a, 24), d_send.at[a])


def local(
    tokens,
    layer_norm_scale,
    input_weight,
    filter_weight,
    filter_bias,
    recur_gate_weight,
    recur_gate_bias,
    input_gate_weight,
    input_gate_bias,
    decay_setting,
    spike_log_decay,
    output_weight,
):
    planes = lax.axis_size("pp") // PLANE
    columns = lax.axis_size("fs")
    length, width = tokens.shape[2:]
    inner = input_weight.shape[2]
    blocks = recur_gate_weight.shape[1]
    dma = pltpu.SemaphoreType.DMA
    hbm = pl.BlockSpec(memory_space=pl.ANY)
    near = pl.BlockSpec(memory_space=pltpu.VMEM)
    bf16, f32 = jnp.bfloat16, jnp.float32
    return pl.pallas_call(
        functools.partial(kernel, planes, columns),
        out_shape=jax.ShapeDtypeStruct(tokens.shape, bf16),
        in_specs=[hbm, near, hbm, near, near, hbm, near, hbm, near, near, near, hbm],
        out_specs=hbm,
        scratch_shapes=[
            pltpu.VMEM((PLANE, width, inner), bf16),
            pltpu.VMEM((PLANE, inner, width), bf16),
            pltpu.VMEM((PLANE, blocks, 128, 256), bf16),
            pltpu.VMEM((PLANE, 16, inner), f32),
            pltpu.VMEM((PLANE, length, 128), f32),
            pltpu.VMEM((length, width), bf16),
            pltpu.VMEM((length, width), bf16),
            pltpu.VMEM((planes, length, width), bf16),
            pltpu.VMEM((planes, length, width), bf16),
            pltpu.VMEM((PLANE, 3 * SUB, inner), f32),
            pltpu.VMEM((PLANE, SUB, inner), f32),
            pltpu.VMEM((length // HALVES, width), bf16),
            pltpu.VMEM((length // HALVES, inner), bf16),
            dma((2, 6, 3)),
            dma((2, 6, 3)),
            dma((3,)),
            dma((2, 3)),
            dma((2, 3)),
            dma((3,)),
            dma((4,)),
            dma((2, 3)),
            dma((2, 3)),
            dma,
            dma((planes, HALVES)),
            dma((planes, HALVES)),
            dma((HALVES,)),
            dma((HALVES,)),
        ],
        compiler_params=pltpu.CompilerParams(
            collective_id=0, has_side_effects=True, vmem_limit_bytes=60 * 1024 * 1024
        ),
    )(
        tokens,
        layer_norm_scale,
        input_weight,
        filter_weight,
        filter_bias,
        recur_gate_weight,
        recur_gate_bias,
        input_gate_weight,
        input_gate_bias,
        decay_setting,
        spike_log_decay,
        output_weight,
    )


def solution(mesh):
    placed = (
        P("pp", ("fs", "tp"), None, None),
        P("pp", None),
        P("pp", None, None),
        P("pp", None, None),
        P("pp", None),
        P("pp", None, None, None),
        P("pp", None),
        P("pp", None, None, None),
        P("pp", None),
        P("pp", None),
        P("pp", None),
        P("pp", None, None),
    )
    return jax.shard_map(
        local,
        mesh=mesh,
        in_specs=placed,
        out_specs=P("pp", ("fs", "tp"), None, None),
        check_vma=False,
    )
```

```python
import functools

import jax
import jax.numpy as jnp
from jax import lax
from jax.experimental import pallas as pl
from jax.experimental.pallas import tpu as pltpu
from jax.sharding import PartitionSpec as P

PLANE = 4
SUB = 8
HALVES = 1
PARTS = 16
MESH = pl.DeviceIdType.MESH


def prepare(hidden, vec, scaled, power):
    length, width = hidden.shape
    inner = vec.shape[1]
    total = jnp.zeros((length, 128), jnp.float32)
    for n in range(width // 128):
        cols = slice(n * 128, (n + 1) * 128)
        row, start = divmod(n * 128, inner)
        part = hidden[:, cols].astype(jnp.float32)
        total = total + part * part
        scaled[:, cols] = (part * vec[row : row + 1, start : start + 128]).astype(jnp.bfloat16)
    power[...] = total


def layer(hidden, win, wout, gates, vec, following, spike, tail, past, scaled, power, states):
    length, width = hidden.shape
    inner = wout.shape[1]
    steps = length // SUB
    top = lax.broadcasted_iota(jnp.int32, (SUB, 128), 0)

    def project(n):
        weight = jnp.concatenate([win[2 * n], win[2 * n + 1]], axis=1)
        return jnp.dot(scaled[...], weight, preferred_element_type=jnp.float32)

    def conv_of(mixed, block):
        cols = slice(block * 128, (block + 1) * 128)
        mixed = (mixed * scale).reshape(steps, SUB, 128)
        taps = [vec[2 + k : 3 + k, cols] for k in range(4)]
        bias = vec[6:7, cols]
        line = []
        for d in range(3):
            rows = slice(d * SUB, (d + 1) * SUB)
            rolled = pltpu.roll(mixed[steps - 3 + d], 1, 0)
            line.append(jnp.where(top == 0, tail[rows, cols], rolled))
            tail[rows, cols] = rolled
        line += [mixed[t] for t in range(steps)]
        conv = jnp.concatenate(
            [
                (bias + sum(line[t + k] * taps[k] for k in range(4)))[None]
                for t in range(steps)
            ],
            axis=0,
        ).reshape(length, 128)
        weight = jnp.concatenate([gates[0, block], gates[1, block]], axis=1)
        pre = jnp.dot(conv.astype(jnp.bfloat16), weight, preferred_element_type=jnp.float32)
        return conv, pre

    def recur(conv, pre, block):
        cols = slice(block * 128, (block + 1) * 128)
        rate = vec[9:10, cols]
        recall = jnp.tanh(pre[:, :128] + vec[7:8, cols]).reshape(steps, SUB, 128)
        inject = jnp.tanh(pre[:, 128:] + vec[8:9, cols]) + 1.0
        decay = jnp.exp2(recall * rate[None] + (spikes + rate[None]))
        room = jnp.maximum(1.0 - decay * decay, 1e-30)
        update = room * lax.rsqrt(room) * (inject * conv).reshape(steps, SUB, 128)
        sums = [update[0]]
        factors = [decay[0]]
        for t in range(1, steps):
            sums.append(decay[t] * sums[-1] + update[t])
            factors.append(decay[t] * factors[-1])
        first = past[:, cols]
        factor = factors[-1]
        last = sums[-1] + jnp.where(top == 0, factor * first, 0.0)
        for hop in (1, 2, 4):
            last = last + factor * jnp.where(top < hop, 0.0, pltpu.roll(last, hop, 0))
            if hop < 4:
                factor = factor * jnp.where(top < hop, 1.0, pltpu.roll(factor, hop, 0))
        ahead = pltpu.roll(last, 1, 0)
        past[:, cols] = ahead
        carry = jnp.where(top == 0, first, ahead)
        done = jnp.concatenate(
            [(sums[t] + factors[t] * carry)[None] for t in range(steps)], axis=0
        )
        states[:, cols] = done.reshape(length, 128).astype(jnp.bfloat16)

    groups = inner // 256
    mixed = project(0)
    scale = lax.rsqrt(jnp.sum(power[...], axis=1, keepdims=True) * (1.0 / width) + 1e-6)
    scale = jnp.broadcast_to(scale, (length, 128))
    spikes = spike[...].reshape(steps, SUB, 128)
    for n in range(groups):
        later = project(n + 1) if n + 1 < groups else None
        left = conv_of(mixed[:, :128], 2 * n)
        right = conv_of(mixed[:, 128:], 2 * n + 1)
        recur(*left, 2 * n)
        recur(*right, 2 * n + 1)
        mixed = later

    total = jnp.zeros((length, 128), jnp.float32)
    for m in range(width // 256):
        weight = jnp.concatenate([wout[2 * m], wout[2 * m + 1]], axis=1)
        projected = jnp.dot(states[...], weight, preferred_element_type=jnp.float32)
        for half in range(2):
            start = m * 256 + half * 128
            cols = slice(start, start + 128)
            part = hidden[:, cols].astype(jnp.float32) + projected[:, half * 128 : half * 128 + 128]
            hidden[:, cols] = part.astype(jnp.bfloat16)
            total = total + part * part
            row, start = divmod(start, inner)
            scaled[:, cols] = (part * following[row : row + 1, start : start + 128]).astype(
                jnp.bfloat16
            )
    power[...] = total


def reorder(src, dst, back):
    length = src.shape[0]
    steps = length // SUB
    row = lax.broadcasted_iota(jnp.int32, (length, length), 0)
    col = lax.broadcasted_iota(jnp.int32, (length, length), 1)
    if back:
        row, col = col, row
    swap = jnp.where(col == lax.rem(row, SUB) * steps + lax.div(row, SUB), 1.0, 0.0)
    swap = swap.astype(jnp.bfloat16)
    for n in range(src.shape[1] // 256):
        cols = slice(n * 256, (n + 1) * 256)
        moved = jnp.dot(swap, src[:, cols], preferred_element_type=jnp.float32)
        dst[:, cols] = moved.astype(jnp.bfloat16)


def kernel(
    planes, columns,
    tok, gain, win, taps, conv_bias, recur_gate, recur_bias, input_gate, input_bias, setting,
    spikes, wout, out,
    win_all, wout_all, gates_all, vec_all, spike_all, raw, home, act, final, tails, pasts,
    scaled, power, states,
    y_recv, x_recv, d_recv, g_recv, y_send, x_send, d_send, g_send, own_sem,
    small_recv, small_send, raw_sem, act_recv, act_send, home_sem, out_recv, lag_sem,
):
    position = lax.axis_index("pp")
    x = lax.axis_index("fs")
    core = lax.axis_index("tp")
    z = position // PLANE
    y = lax.rem(position, PLANE)
    parity = lax.rem(x, 2)
    length, width = raw.shape
    inner = wout_all.shape[2]
    chunk = length // HALVES

    def at_y(by):
        return z * PLANE + lax.rem(y + by, PLANE)

    def plane_slot(by):
        return lax.rem(y + by, PLANE)

    def rows_of(half):
        return pl.ds(pl.multiple_of(half * chunk, chunk), chunk)

    up, down, across = {"pp": at_y(1)}, {"pp": at_y(3)}, {"pp": at_y(2)}
    right, left = {"fs": lax.rem(x + 1, columns)}, {"fs": lax.rem(x + columns - 1, columns)}
    sibling = {"tp": 1 - core}
    z_peers = [{"pp": lax.rem(z + by, planes) * PLANE + y} for by in range(1, planes)]

    own = [
        pltpu.make_async_copy(source.at[0], gates_all.at[y, n], own_sem.at[n])
        for n, source in enumerate((recur_gate, input_gate))
    ]
    for copy in own:
        copy.start()
    pltpu.make_async_copy(tok.at[0, 0], raw, raw_sem).start()

    barrier = pltpu.get_barrier_semaphore()
    peers = [up, down, across, right, left, sibling] + z_peers
    for peer in peers:
        pl.semaphore_signal(barrier, inc=1, device_id=peer, device_id_type=MESH)

    vec_all[y, 0:1] = gain[:, :inner]
    vec_all[y, 1:2] = gain[:, inner:]
    log2e = 1.4426950408889634
    vec_all[y, 2:6] = 0.5 * taps[0]
    vec_all[y, 6:7] = 0.5 * conv_bias[...]
    vec_all[y, 7:8] = 0.5 * recur_bias[...]
    vec_all[y, 8:9] = 0.5 * input_bias[...]
    below = -setting[...]
    softplus = jnp.maximum(below, 0.0) + jnp.log1p(jnp.exp(-jnp.abs(below)))
    vec_all[y, 9:10] = (-4.0 * log2e) * softplus
    row = lax.broadcasted_iota(jnp.int32, (length, length), 0)
    col = lax.broadcasted_iota(jnp.int32, (length, length), 1)
    within = lax.rem(row, chunk)
    token = (row - within) + lax.rem(within, SUB) * (chunk // SUB) + lax.div(within, SUB)
    picked = jnp.sum(jnp.where(col == token, spikes[...], 0.0), axis=1, keepdims=True)
    spike_all[y] = jnp.broadcast_to(picked * log2e, (length, 128))

    pl.semaphore_wait(barrier, len(peers))

    gathered = (win_all, wout_all)

    def piece(a, slot, index):
        if a == 1:
            return wout_all.at[slot, index]
        half = win_all.shape[2] // 2
        return win_all.at[slot, index // 2, pl.ds(pl.multiple_of(lax.rem(index, 2) * half, half), half)]

    def source(a, index):
        if a == 1:
            return wout.at[0, :, pl.ds(pl.multiple_of(index * 128, 128), 128)]
        half = win_all.shape[2] // 2
        return win.at[
            0,
            pl.ds(pl.multiple_of(lax.rem(index, 2) * half, half), half),
            pl.ds(pl.multiple_of(index // 2 * 128, 128), 128),
        ]

    def gate_piece(slot, index):
        return gates_all.at[slot, :, pl.ds(4 * core + 2 * index, 2)]

    def push(src, dst, send_sem, recv_sem, to):
        pltpu.make_async_remote_copy(
            src_ref=src, dst_ref=dst, send_sem=send_sem, recv_sem=recv_sem,
            device_id=to, device_id_type=MESH,
        ).start()

    def send(a, src, slot, index, send_sem, recv_sem, to):
        push(src, piece(a, slot, index), send_sem, recv_sem, to)

    def await_bytes(ref, sem):
        pltpu.make_async_copy(ref, ref, sem).wait()

    def pieces_of(a, count):
        tiles = count // 2 if a == 0 else count
        if count == 6:
            return gathered[a].at[0, pl.ds(0, tiles)]
        return gathered[a].at[pl.ds(0, 2), pl.ds(0, tiles // 2)]

    mine = 8 * parity + 4 * core
    other = 8 * (1 - parity) + 4 * core

    for unit in range(4):
        for a in range(2):
            j = unit
            send(a, source(a, mine + j), y, mine + j,
                 y_send.at[0, a], y_recv.at[0, unit, a], up)
            j = (unit + 2) % 4
            send(a, source(a, mine + j), y, mine + j,
                 y_send.at[1, a], y_recv.at[1, unit, a], down)
    smalls = (vec_all, spike_all)
    for n, ref in enumerate(smalls):
        for by in range(1, 4):
            pltpu.make_async_remote_copy(
                src_ref=ref.at[y], dst_ref=ref.at[y], send_sem=small_send.at[n, by - 1],
                recv_sem=small_recv.at[n, by - 1],
                device_id={"pp": at_y(by)}, device_id_type=MESH,
            ).start()
    for n in range(win_all.shape[1]):
        pltpu.make_async_copy(
            win.at[0, :, n * 128 : (n + 1) * 128], win_all.at[y, n], own_sem.at[2]
        ).start()
    for n in range(wout_all.shape[1]):
        pltpu.make_async_copy(
            wout.at[0, :, n * 128 : (n + 1) * 128], wout_all.at[y, n], own_sem.at[3]
        ).start()

    await_bytes(raw, raw_sem)
    for half in range(HALVES):
        rows = slice(half * chunk, (half + 1) * chunk)
        reorder(raw.at[rows], home.at[rows], False)

        @pl.when(z != 0)
        def _():
            pltpu.make_async_remote_copy(
                src_ref=home.at[rows], dst_ref=act.at[z, rows], send_sem=home_sem.at[half],
                recv_sem=act_recv.at[z, half],
                device_id={"pp": y}, device_id_type=MESH,
            ).start()

        @pl.when(z == 0)
        def _():
            pltpu.make_async_copy(home.at[rows], act.at[0, rows], act_recv.at[0, half]).start()

    def arrivals(unit):
        from_below = (plane_slot(3), unit) if unit < 4 else (plane_slot(2), unit - 4)
        from_above = (plane_slot(1), (unit + 2) % 4) if unit < 4 else (plane_slot(2), unit - 2)
        return from_below, from_above

    x_units = []
    for unit in range(6):
        below, above = arrivals(unit)
        x_units.append((below, above) if below[1] < 2 else (above, below))

    def relay_y(unit, a):
        for side, (slot, j) in enumerate(arrivals(unit)):
            ref = piece(a, slot, mine + j)
            await_bytes(ref, y_recv.at[side, unit, a])
            if unit < 2:
                send(a, ref, slot, mine + j, y_send.at[side, a],
                     y_recv.at[side, 4 + unit, a], up if side == 0 else down)
            x_side = 0 if j < 2 else 1
            send(a, ref, slot, mine + j, x_send.at[x_side, a],
                 x_recv.at[x_side, unit, a], left if x_side == 0 else right)
            send(a, ref, slot, mine + j, d_send.at[a], d_recv.at[a], sibling)

    def relay_x(unit, a):
        for side, (slot, j) in enumerate(x_units[unit]):
            ref = piece(a, slot, other + j)
            await_bytes(ref, x_recv.at[side, unit, a])
            send(a, ref, slot, other + j, d_send.at[a], d_recv.at[a], sibling)

    def relay_gates(n):
        slots = ((3, 0), (3, 1), (2, 0)), ((1, 1), (1, 0), (2, 1))
        for side in range(2):
            by, index = slots[side][n]
            ref = gate_piece(plane_slot(by), index)
            await_bytes(ref, g_recv.at[side, n])
            if n == 0:
                push(ref, ref, g_send.at[side], g_recv.at[side, 2], up if side == 0 else down)
            push(ref, ref, d_send.at[2], d_recv.at[2], sibling)

    for unit in range(6):
        for a in range(2):
            relay_y(unit, a)
            if unit > 0:
                relay_x(unit - 1, a)
        if unit == 1:
            for copy in own:
                copy.wait()
            for n in range(2):
                for side, to in enumerate((up, down)):
                    ref = gate_piece(y, n if side == 0 else 1 - n)
                    push(ref, ref, g_send.at[side], g_recv.at[side, n], to)
    for n in range(3):
        relay_gates(n)
    for a in range(2):
        relay_x(5, a)

    await_bytes(win_all.at[y], own_sem.at[2])
    await_bytes(wout_all.at[y], own_sem.at[3])
    for n, ref in enumerate(smalls):
        for by in range(1, 4):
            await_bytes(ref.at[plane_slot(4 - by)], small_recv.at[n, by - 1])
    for a in range(2):
        await_bytes(pieces_of(a, 24), d_recv.at[a])
    await_bytes(gates_all.at[pl.ds(0, 3), :, pl.ds(0, 4)], d_recv.at[2])

    def micro(step, token):
        i = step // HALVES
        half = lax.rem(step, HALVES)
        rows = rows_of(half)
        here = act.at[i, rows]
        await_bytes(here, act_recv.at[i, half])

        @pl.when(half == 0)
        def _():
            tails[...] = jnp.zeros_like(tails)
            pasts[...] = jnp.zeros_like(pasts)

        @pl.when((z == 0) & (core == 1) & (step == 0))
        def _():
            pl.semaphore_wait(lag_sem, 1)

        prepare(here, vec_all.at[0], scaled, power)

        def one(s, token):
            layer(here, win_all.at[s], wout_all.at[s], gates_all.at[s], vec_all.at[s],
                  vec_all.at[lax.rem(s + 1, PLANE)], spike_all.at[s, rows], tails.at[s],
                  pasts.at[s], scaled, power, states)

            @pl.when((z == 0) & (core == 0) & (step == 0) & (s == 2))
            def _():
                pl.semaphore_signal(lag_sem, inc=1, device_id=sibling, device_id_type=MESH)

            return token

        lax.fori_loop(0, PLANE, one, 0)

        @pl.when(z < planes - 1)
        def _():
            pltpu.make_async_remote_copy(
                src_ref=here, dst_ref=here, send_sem=act_send.at[i, half],
                recv_sem=act_recv.at[i, half],
                device_id={"pp": lax.rem(z + 1, planes) * PLANE + y}, device_id_type=MESH,
            ).start()

        @pl.when(z == planes - 1)
        def _():
            reorder(here, final.at[i, rows], True)

            @pl.when(i < planes - 1)
            def _():
                pltpu.make_async_remote_copy(
                    src_ref=final.at[i, rows], dst_ref=out.at[0, 0, rows],
                    send_sem=act_send.at[i, half], recv_sem=out_recv.at[half],
                    device_id={"pp": i * PLANE + y}, device_id_type=MESH,
                ).start()

            @pl.when(i == planes - 1)
            def _():
                pltpu.make_async_copy(
                    final.at[i, rows], out.at[0, 0, rows], out_recv.at[half]
                ).start()

        return token

    lax.fori_loop(0, planes * HALVES, micro, 0)

    for half in range(HALVES):
        rows = slice(half * chunk, (half + 1) * chunk)
        await_bytes(out.at[0, 0, rows], out_recv.at[half])
        for i in range(planes):
            if i < planes - 1:
                await_bytes(act.at[i, rows], act_send.at[i, half])
            else:
                @pl.when(z < planes - 1)
                def _():
                    await_bytes(act.at[i, rows], act_send.at[i, half])

        @pl.when(z != 0)
        def _():
            await_bytes(home.at[rows], home_sem.at[half])

    for n, ref in enumerate(smalls):
        for by in range(1, 4):
            await_bytes(ref.at[y], small_send.at[n, by - 1])
    for side in range(2):
        for a in range(2):
            await_bytes(pieces_of(a, 6), y_send.at[side, a])
            await_bytes(pieces_of(a, 6), x_send.at[side, a])
        await_bytes(gates_all.at[pl.ds(0, 3), :, pl.ds(0, 2)], g_send.at[side])
    for a in range(2):
        await_bytes(pieces_of(a, 24), d_send.at[a])
    await_bytes(gates_all.at[pl.ds(0, 3), :, pl.ds(0, 4)], d_send.at[2])


def local(
    tokens,
    layer_norm_scale,
    input_weight,
    filter_weight,
    filter_bias,
    recur_gate_weight,
    recur_gate_bias,
    input_gate_weight,
    input_gate_bias,
    decay_setting,
    spike_log_decay,
    output_weight,
):
    planes = lax.axis_size("pp") // PLANE
    columns = lax.axis_size("fs")
    length, width = tokens.shape[2:]
    inner = input_weight.shape[2]
    blocks = recur_gate_weight.shape[1]
    dma = pltpu.SemaphoreType.DMA
    hbm = pl.BlockSpec(memory_space=pl.ANY)
    near = pl.BlockSpec(memory_space=pltpu.VMEM)
    bf16, f32 = jnp.bfloat16, jnp.float32
    return pl.pallas_call(
        functools.partial(kernel, planes, columns),
        out_shape=jax.ShapeDtypeStruct(tokens.shape, bf16),
        in_specs=[hbm, near, hbm, near, near, hbm, near, hbm, near, near, near, hbm],
        out_specs=hbm,
        scratch_shapes=[
            pltpu.VMEM((PLANE, inner // 128, width, 128), bf16),
            pltpu.VMEM((PLANE, width // 128, inner, 128), bf16),
            pltpu.VMEM((PLANE, 2, blocks, 128, 128), bf16),
            pltpu.VMEM((PLANE, 16, inner), f32),
            pltpu.VMEM((PLANE, length, 128), f32),
            pltpu.VMEM((length, width), bf16),
            pltpu.VMEM((length, width), bf16),
            pltpu.VMEM((planes, length, width), bf16),
            pltpu.VMEM((planes, length, width), bf16),
            pltpu.VMEM((PLANE, 3 * SUB, inner), f32),
            pltpu.VMEM((PLANE, SUB, inner), f32),
            pltpu.VMEM((length // HALVES, width), bf16),
            pltpu.VMEM((length // HALVES, 128), f32),
            pltpu.VMEM((length // HALVES, inner), bf16),
            dma((2, 6, 2)),
            dma((2, 6, 2)),
            dma((3,)),
            dma((2, 3)),
            dma((2, 2)),
            dma((2, 2)),
            dma((3,)),
            dma((2,)),
            dma((4,)),
            dma((2, 3)),
            dma((2, 3)),
            dma,
            dma((planes, HALVES)),
            dma((planes, HALVES)),
            dma((HALVES,)),
            dma((HALVES,)),
            pltpu.SemaphoreType.REGULAR,
        ],
        compiler_params=pltpu.CompilerParams(
            collective_id=0, has_side_effects=True, vmem_limit_bytes=60 * 1024 * 1024
        ),
    )(
        tokens,
        layer_norm_scale,
        input_weight,
        filter_weight,
        filter_bias,
        recur_gate_weight,
        recur_gate_bias,
        input_gate_weight,
        input_gate_bias,
        decay_setting,
        spike_log_decay,
        output_weight,
    )


def solution(mesh):
    placed = (
        P("pp", ("fs", "tp"), None, None),
        P("pp", None),
        P("pp", None, None),
        P("pp", None, None),
        P("pp", None),
        P("pp", None, None, None),
        P("pp", None),
        P("pp", None, None, None),
        P("pp", None),
        P("pp", None),
        P("pp", None),
        P("pp", None, None),
    )
    return jax.shard_map(
        local,
        mesh=mesh,
        in_specs=placed,
        out_specs=P("pp", ("fs", "tp"), None, None),
        check_vma=False,
    )
```

```python
import functools

import jax
import jax.numpy as jnp
from jax import lax
from jax.experimental import pallas as pl
from jax.experimental.pallas import tpu as pltpu
from jax.sharding import PartitionSpec as P

PLANE = 4
SUB = 8
HALVES = 1
PARTS = 16
MESH = pl.DeviceIdType.MESH


def prepare(hidden, vec, scaled, power):
    length, width = hidden.shape
    inner = vec.shape[1]
    total = jnp.zeros((length, 128), jnp.float32)
    for n in range(width // 128):
        cols = slice(n * 128, (n + 1) * 128)
        row, start = divmod(n * 128, inner)
        part = hidden[:, cols].astype(jnp.float32)
        total = total + part * part
        scaled[:, cols] = (part * vec[row : row + 1, start : start + 128]).astype(jnp.bfloat16)
    power[...] = total


def layer(hidden, win, wout, gates, vec, following, spike, tail, past, scaled, power, states):
    length, width = hidden.shape
    inner = wout.shape[1]
    steps = length // SUB
    top = lax.broadcasted_iota(jnp.int32, (SUB, 128), 0)

    def project(n):
        weight = jnp.concatenate([win[2 * n], win[2 * n + 1]], axis=1)
        return jnp.dot(scaled[...], weight, preferred_element_type=jnp.float32)

    def conv_of(mixed, block):
        cols = slice(block * 128, (block + 1) * 128)
        mixed = (mixed * scale).reshape(steps, SUB, 128)
        taps = [vec[2 + k : 3 + k, cols] for k in range(4)]
        bias = vec[6:7, cols]
        line = []
        for d in range(3):
            rows = slice(d * SUB, (d + 1) * SUB)
            rolled = pltpu.roll(mixed[steps - 3 + d], 1, 0)
            line.append(jnp.where(top == 0, tail[rows, cols], rolled))
            tail[rows, cols] = rolled
        line += [mixed[t] for t in range(steps)]
        conv = jnp.concatenate(
            [
                (bias + sum(line[t + k] * taps[k] for k in range(4)))[None]
                for t in range(steps)
            ],
            axis=0,
        ).reshape(length, 128)
        weight = jnp.concatenate([gates[0, block], gates[1, block]], axis=1)
        pre = jnp.dot(conv.astype(jnp.bfloat16), weight, preferred_element_type=jnp.float32)
        return conv, pre

    def recur(conv, pre, block):
        cols = slice(block * 128, (block + 1) * 128)
        rate = vec[9:10, cols]
        recall = jnp.tanh(pre[:, :128] + vec[7:8, cols]).reshape(steps, SUB, 128)
        inject = jnp.tanh(pre[:, 128:] + vec[8:9, cols]) + 1.0
        decay = jnp.exp2(recall * rate[None] + (spikes + rate[None]))
        room = jnp.maximum(1.0 - decay * decay, 1e-30)
        update = room * lax.rsqrt(room) * (inject * conv).reshape(steps, SUB, 128)
        sums = [update[0]]
        factors = [decay[0]]
        for t in range(1, steps):
            sums.append(decay[t] * sums[-1] + update[t])
            factors.append(decay[t] * factors[-1])
        first = past[:, cols]
        factor = factors[-1]
        last = sums[-1] + jnp.where(top == 0, factor * first, 0.0)
        for hop in (1, 2, 4):
            last = last + factor * jnp.where(top < hop, 0.0, pltpu.roll(last, hop, 0))
            if hop < 4:
                factor = factor * jnp.where(top < hop, 1.0, pltpu.roll(factor, hop, 0))
        ahead = pltpu.roll(last, 1, 0)
        past[:, cols] = ahead
        carry = jnp.where(top == 0, first, ahead)
        done = jnp.concatenate(
            [(sums[t] + factors[t] * carry)[None] for t in range(steps)], axis=0
        )
        states[:, cols] = done.reshape(length, 128).astype(jnp.bfloat16)

    groups = inner // 256
    mixed = project(0)
    scale = lax.rsqrt(jnp.sum(power[...], axis=1, keepdims=True) * (1.0 / width) + 1e-6)
    scale = jnp.broadcast_to(scale, (length, 128))
    spikes = spike[...].reshape(steps, SUB, 128)
    for n in range(groups):
        later = project(n + 1) if n + 1 < groups else None
        left = conv_of(mixed[:, :128], 2 * n)
        right = conv_of(mixed[:, 128:], 2 * n + 1)
        recur(*left, 2 * n)
        recur(*right, 2 * n + 1)
        mixed = later

    total = jnp.zeros((length, 128), jnp.float32)
    for m in range(width // 256):
        weight = jnp.concatenate([wout[2 * m], wout[2 * m + 1]], axis=1)
        projected = jnp.dot(states[...], weight, preferred_element_type=jnp.float32)
        for half in range(2):
            start = m * 256 + half * 128
            cols = slice(start, start + 128)
            part = hidden[:, cols].astype(jnp.float32) + projected[:, half * 128 : half * 128 + 128]
            hidden[:, cols] = part.astype(jnp.bfloat16)
            total = total + part * part
            row, start = divmod(start, inner)
            scaled[:, cols] = (part * following[row : row + 1, start : start + 128]).astype(
                jnp.bfloat16
            )
    power[...] = total


def reorder(src, dst, back):
    length = src.shape[0]
    steps = length // SUB
    row = lax.broadcasted_iota(jnp.int32, (length, length), 0)
    col = lax.broadcasted_iota(jnp.int32, (length, length), 1)
    if back:
        row, col = col, row
    swap = jnp.where(col == lax.rem(row, SUB) * steps + lax.div(row, SUB), 1.0, 0.0)
    swap = swap.astype(jnp.bfloat16)
    for n in range(src.shape[1] // 256):
        cols = slice(n * 256, (n + 1) * 256)
        moved = jnp.dot(swap, src[:, cols], preferred_element_type=jnp.float32)
        dst[:, cols] = moved.astype(jnp.bfloat16)


def kernel(
    planes, columns,
    tok, gain, win, taps, conv_bias, recur_gate, recur_bias, input_gate, input_bias, setting,
    spikes, wout, out,
    win_all, wout_all, gates_all, vec_all, spike_all, raw, home, act, final, tails, pasts,
    scaled, power, states, relay_wout, relay_gate,
    onward_wout, onward_gate,
    y_recv, x_recv, d_recv, g_recv, y_send, x_send, d_send, g_send, own_sem,
    small_recv, small_send, raw_sem, act_recv, act_send, home_sem, out_recv, lag_sem,
    f_send, f_recv, h_send, h_recv, k_send, k_recv,
):
    position = lax.axis_index("pp")
    x = lax.axis_index("fs")
    core = lax.axis_index("tp")
    z = position // PLANE
    y = lax.rem(position, PLANE)
    parity = lax.rem(x, 2)
    length, width = raw.shape
    inner = wout_all.shape[2]
    chunk = length // HALVES

    def at_y(by):
        return z * PLANE + lax.rem(y + by, PLANE)

    def plane_slot(by):
        return lax.rem(y + by, PLANE)

    def rows_of(half):
        return pl.ds(pl.multiple_of(half * chunk, chunk), chunk)

    up, down, across = {"pp": at_y(1)}, {"pp": at_y(3)}, {"pp": at_y(2)}
    right, left = {"fs": lax.rem(x + 1, columns)}, {"fs": lax.rem(x + columns - 1, columns)}
    sibling = {"tp": 1 - core}
    z_peers = [{"pp": lax.rem(z + by, planes) * PLANE + y} for by in range(1, planes)]

    own = [
        pltpu.make_async_copy(source.at[0], gates_all.at[y, n], own_sem.at[n])
        for n, source in enumerate((recur_gate, input_gate))
    ]
    for copy in own:
        copy.start()
    pltpu.make_async_copy(tok.at[0, 0], raw, raw_sem).start()

    barrier = pltpu.get_barrier_semaphore()
    mirror = [{"pp": (planes - 1 - z) * PLANE + lax.rem(y + by, PLANE)} for by in range(1, 4)]
    peers = [up, down, across, right, left, sibling] + z_peers + mirror
    for peer in peers:
        pl.semaphore_signal(barrier, inc=1, device_id=peer, device_id_type=MESH)

    vec_all[y, 0:1] = gain[:, :inner]
    vec_all[y, 1:2] = gain[:, inner:]
    log2e = 1.4426950408889634
    vec_all[y, 2:6] = 0.5 * taps[0]
    vec_all[y, 6:7] = 0.5 * conv_bias[...]
    vec_all[y, 7:8] = 0.5 * recur_bias[...]
    vec_all[y, 8:9] = 0.5 * input_bias[...]
    below = -setting[...]
    softplus = jnp.maximum(below, 0.0) + jnp.log1p(jnp.exp(-jnp.abs(below)))
    vec_all[y, 9:10] = (-4.0 * log2e) * softplus
    row = lax.broadcasted_iota(jnp.int32, (length, length), 0)
    col = lax.broadcasted_iota(jnp.int32, (length, length), 1)
    within = lax.rem(row, chunk)
    token = (row - within) + lax.rem(within, SUB) * (chunk // SUB) + lax.div(within, SUB)
    picked = jnp.sum(jnp.where(col == token, spikes[...], 0.0), axis=1, keepdims=True)
    spike_all[y] = jnp.broadcast_to(picked * log2e, (length, 128))

    pl.semaphore_wait(barrier, len(peers))

    gathered = (win_all, wout_all)

    def piece(a, slot, index):
        if a == 1:
            return wout_all.at[slot, index]
        half = win_all.shape[2] // 2
        return win_all.at[slot, index // 2, pl.ds(pl.multiple_of(lax.rem(index, 2) * half, half), half)]

    def source(a, index):
        if a == 1:
            return wout.at[0, :, pl.ds(pl.multiple_of(index * 128, 128), 128)]
        half = win_all.shape[2] // 2
        return win.at[
            0,
            pl.ds(pl.multiple_of(lax.rem(index, 2) * half, half), half),
            pl.ds(pl.multiple_of(index // 2 * 128, 128), 128),
        ]

    def gate_piece(slot, index):
        return gates_all.at[slot, :, pl.ds(4 * core + 2 * index, 2)]

    def push(src, dst, send_sem, recv_sem, to):
        pltpu.make_async_remote_copy(
            src_ref=src, dst_ref=dst, send_sem=send_sem, recv_sem=recv_sem,
            device_id=to, device_id_type=MESH,
        ).start()

    def send(a, src, slot, index, send_sem, recv_sem, to):
        push(src, piece(a, slot, index), send_sem, recv_sem, to)

    def await_bytes(ref, sem):
        pltpu.make_async_copy(ref, ref, sem).wait()

    def pieces_of(a, count):
        tiles = count // 2 if a == 0 else count
        if count == 6:
            return gathered[a].at[0, pl.ds(0, tiles)]
        return gathered[a].at[pl.ds(0, 2), pl.ds(0, tiles // 2)]

    mine = 8 * parity + 4 * core
    other = 8 * (1 - parity) + 4 * core

    first, last = z == 0, z == planes - 1
    lower = pl.ds(wout_all.shape[2] // 2, wout_all.shape[2] // 2)
    upper = pl.ds(0, wout_all.shape[2] // 2)
    detours = [(8 * side + 4 * core + j) for side in range(2) for j in (1, 3)]
    core_gates = pl.ds(4 * core, 4)

    for copy in own:
        copy.wait()

    @pl.when(first)
    def _():
        to = {"pp": (planes - 1) * PLANE + y}
        for n, index in enumerate(detours):
            column = pl.ds(pl.multiple_of(index * 128, 128), 128)
            push(wout.at[0, lower, column], relay_wout.at[n], f_send.at[0], f_recv.at[n], to)
        push(gates_all.at[y, :, core_gates], relay_gate, f_send.at[1], f_recv.at[4], to)

    def split(a, j, act_on):
        if a == 0 or j % 2 == 0:
            act_on(lambda ref: ref)
            return

        @pl.when(first)
        def _():
            act_on(lambda ref: ref.at[upper])

        @pl.when(z != 0)
        def _():
            act_on(lambda ref: ref)

    def start_unit(unit):
        for a in range(2):
            for side, to in enumerate((up, down)):
                j = (unit + 2 * side) % 4
                split(a, j, lambda cut: push(
                    cut(source(a, mine + j)), cut(piece(a, y, mine + j)),
                    y_send.at[side, a], y_recv.at[side, unit, a], to))

    start_unit(0)

    def detour(slot, n):
        return wout_all.at[slot, detours[n], lower] if n < 4 else gates_all.at[slot, :, core_gates]

    headings = (3, 1, 1, 1, 3)

    @pl.when(last)
    def _():
        for n, heading in enumerate(headings):
            ref, store = (relay_wout.at[n], onward_wout.at[n]) if n < 4 else (relay_gate, onward_gate)
            await_bytes(ref, f_recv.at[n])
            push(ref, store, k_send.at[n // 4], k_recv.at[n], {"pp": at_y(heading)})
            by = 4 - heading
            push(ref, detour(y, n), h_send.at[n // 4], h_recv.at[by - 1, n],
                 {"pp": lax.rem(y + by, PLANE)})

    start_unit(1)

    @pl.when(last)
    def _():
        for n, heading in enumerate(headings):
            ref = onward_wout.at[n] if n < 4 else onward_gate
            await_bytes(ref, k_recv.at[n])
            dst = detour(plane_slot(4 - heading), n)
            push(ref, dst, h_send.at[n // 4], h_recv.at[1, n],
                 {"pp": lax.rem(y + heading, PLANE)})
            push(ref, dst, h_send.at[n // 4], h_recv.at[heading - 1, n], {"pp": y})

    start_unit(2)
    start_unit(3)
    smalls = (vec_all, spike_all)
    for n, ref in enumerate(smalls):
        for by in range(1, 4):
            pltpu.make_async_remote_copy(
                src_ref=ref.at[y], dst_ref=ref.at[y], send_sem=small_send.at[n, by - 1],
                recv_sem=small_recv.at[n, by - 1],
                device_id={"pp": at_y(by)}, device_id_type=MESH,
            ).start()
    for n in range(win_all.shape[1]):
        pltpu.make_async_copy(
            win.at[0, :, n * 128 : (n + 1) * 128], win_all.at[y, n], own_sem.at[2]
        ).start()
    for n in range(wout_all.shape[1]):
        pltpu.make_async_copy(
            wout.at[0, :, n * 128 : (n + 1) * 128], wout_all.at[y, n], own_sem.at[3]
        ).start()

    await_bytes(raw, raw_sem)
    for half in range(HALVES):
        rows = slice(half * chunk, (half + 1) * chunk)
        reorder(raw.at[rows], home.at[rows], False)

        @pl.when(z == 0)
        def _():
            pltpu.make_async_copy(home.at[rows], act.at[0, rows], act_recv.at[0, half]).start()

    def send_home():
        for half in range(HALVES):
            rows = slice(half * chunk, (half + 1) * chunk)
            push(home.at[rows], act.at[z, rows], home_sem.at[half], act_recv.at[z, half], {"pp": y})

    pl.when((z == 1) | last)(send_home)

    def arrivals(unit):
        from_below = (plane_slot(3), unit) if unit < 4 else (plane_slot(2), unit - 4)
        from_above = (plane_slot(1), (unit + 2) % 4) if unit < 4 else (plane_slot(2), unit - 2)
        return from_below, from_above

    x_units = []
    for unit in range(6):
        below, above = arrivals(unit)
        x_units.append((below, above) if below[1] < 2 else (above, below))

    def relay_y(unit, a):
        for side, (slot, j) in enumerate(arrivals(unit)):
            def forward(cut):
                ref = cut(piece(a, slot, mine + j))
                await_bytes(ref, y_recv.at[side, unit, a])
                if unit < 2:
                    push(ref, ref, y_send.at[side, a], y_recv.at[side, 4 + unit, a],
                         up if side == 0 else down)
                x_side = 0 if j < 2 else 1
                push(ref, ref, x_send.at[x_side, a], x_recv.at[x_side, unit, a],
                     left if x_side == 0 else right)
                push(ref, ref, d_send.at[a], d_recv.at[a], sibling)

            split(a, j, forward)

    def relay_x(unit, a):
        for side, (slot, j) in enumerate(x_units[unit]):
            def forward(cut):
                ref = cut(piece(a, slot, other + j))
                await_bytes(ref, x_recv.at[side, unit, a])
                push(ref, ref, d_send.at[a], d_recv.at[a], sibling)

            split(a, j, forward)

    def relay_gates(n):
        slots = ((3, 0), (3, 1), (2, 0)), ((1, 1), (1, 0), (2, 1))
        for side in range(2):
            by, index = slots[side][n]
            ref = gate_piece(plane_slot(by), index)
            await_bytes(ref, g_recv.at[side, n])
            if n == 0:
                push(ref, ref, g_send.at[side], g_recv.at[side, 2], up if side == 0 else down)
            push(ref, ref, d_send.at[2], d_recv.at[2], sibling)

    for unit in range(6):
        for a in range(2):
            relay_y(unit, a)
            if unit > 0:
                relay_x(unit - 1, a)
        if unit == 4:
            pl.when((z > 1) & (z != planes - 1))(send_home)
        if unit == 1:
            @pl.when(z != 0)
            def _():
                for n in range(2):
                    for side, to in enumerate((up, down)):
                        ref = gate_piece(y, n if side == 0 else 1 - n)
                        push(ref, ref, g_send.at[side], g_recv.at[side, n], to)

    @pl.when(z != 0)
    def _():
        for n in range(3):
            relay_gates(n)

    @pl.when(first)
    def _():
        for n in range(5):
            for by in range(1, 4):
                slot = plane_slot(4 - by)
                ref = detour(slot, n)
                await_bytes(ref, h_recv.at[by - 1, n])
                push(ref, ref, d_send.at[1 + n // 4], d_recv.at[1 + n // 4], sibling)

    for a in range(2):
        relay_x(5, a)

    await_bytes(win_all.at[y], own_sem.at[2])
    await_bytes(wout_all.at[y], own_sem.at[3])
    for n, ref in enumerate(smalls):
        for by in range(1, 4):
            await_bytes(ref.at[plane_slot(4 - by)], small_recv.at[n, by - 1])
    for a in range(2):
        await_bytes(pieces_of(a, 24), d_recv.at[a])
    await_bytes(gates_all.at[pl.ds(0, 3), :, pl.ds(0, 4)], d_recv.at[2])

    def micro(step, token):
        i = step // HALVES
        half = lax.rem(step, HALVES)
        rows = rows_of(half)
        here = act.at[i, rows]
        await_bytes(here, act_recv.at[i, half])

        @pl.when(half == 0)
        def _():
            tails[...] = jnp.zeros_like(tails)
            pasts[...] = jnp.zeros_like(pasts)

        @pl.when((z == 0) & (core == 1) & (step == 0))
        def _():
            pl.semaphore_wait(lag_sem, 1)

        prepare(here, vec_all.at[0], scaled, power)

        def one(s, token):
            layer(here, win_all.at[s], wout_all.at[s], gates_all.at[s], vec_all.at[s],
                  vec_all.at[lax.rem(s + 1, PLANE)], spike_all.at[s, rows], tails.at[s],
                  pasts.at[s], scaled, power, states)

            @pl.when((z == 0) & (core == 0) & (step == 0) & (s == 2))
            def _():
                pl.semaphore_signal(lag_sem, inc=1, device_id=sibling, device_id_type=MESH)

            return token

        lax.fori_loop(0, PLANE, one, 0)

        @pl.when(z < planes - 1)
        def _():
            pltpu.make_async_remote_copy(
                src_ref=here, dst_ref=here, send_sem=act_send.at[i, half],
                recv_sem=act_recv.at[i, half],
                device_id={"pp": lax.rem(z + 1, planes) * PLANE + y}, device_id_type=MESH,
            ).start()

        @pl.when(z == planes - 1)
        def _():
            reorder(here, final.at[i, rows], True)

            @pl.when(i < planes - 1)
            def _():
                pltpu.make_async_remote_copy(
                    src_ref=final.at[i, rows], dst_ref=out.at[0, 0, rows],
                    send_sem=act_send.at[i, half], recv_sem=out_recv.at[half],
                    device_id={"pp": i * PLANE + y}, device_id_type=MESH,
                ).start()

            @pl.when(i == planes - 1)
            def _():
                pltpu.make_async_copy(
                    final.at[i, rows], out.at[0, 0, rows], out_recv.at[half]
                ).start()

        return token

    lax.fori_loop(0, planes * HALVES, micro, 0)

    for half in range(HALVES):
        rows = slice(half * chunk, (half + 1) * chunk)
        await_bytes(out.at[0, 0, rows], out_recv.at[half])
        for i in range(planes):
            if i < planes - 1:
                await_bytes(act.at[i, rows], act_send.at[i, half])
            else:
                @pl.when(z < planes - 1)
                def _():
                    await_bytes(act.at[i, rows], act_send.at[i, half])

        @pl.when(z != 0)
        def _():
            await_bytes(home.at[rows], home_sem.at[half])

    for n, ref in enumerate(smalls):
        for by in range(1, 4):
            await_bytes(ref.at[y], small_send.at[n, by - 1])
    for side in range(2):
        for sem in (y_send, x_send):
            await_bytes(pieces_of(0, 6), sem.at[side, 0])

            @pl.when(first)
            def _():
                await_bytes(wout_all.at[0, pl.ds(0, 9), upper], sem.at[side, 1])

            @pl.when(z != 0)
            def _():
                await_bytes(pieces_of(1, 6), sem.at[side, 1])

        @pl.when(z != 0)
        def _():
            await_bytes(gates_all.at[pl.ds(0, 3), :, pl.ds(0, 2)], g_send.at[side])

    @pl.when(first)
    def _():
        await_bytes(relay_wout, f_send.at[0])
        await_bytes(relay_gate, f_send.at[1])

    @pl.when(last)
    def _():
        await_bytes(onward_wout, k_send.at[0])
        await_bytes(onward_gate, k_send.at[1])
        await_bytes(wout_all.at[0, pl.ds(0, 12), upper], h_send.at[0])
        await_bytes(gates_all.at[pl.ds(0, 3), :, pl.ds(0, 4)], h_send.at[1])

    for a in range(2):
        await_bytes(pieces_of(a, 24), d_send.at[a])
    await_bytes(gates_all.at[pl.ds(0, 3), :, pl.ds(0, 4)], d_send.at[2])


def local(
    tokens,
    layer_norm_scale,
    input_weight,
    filter_weight,
    filter_bias,
    recur_gate_weight,
    recur_gate_bias,
    input_gate_weight,
    input_gate_bias,
    decay_setting,
    spike_log_decay,
    output_weight,
):
    planes = lax.axis_size("pp") // PLANE
    columns = lax.axis_size("fs")
    length, width = tokens.shape[2:]
    inner = input_weight.shape[2]
    blocks = recur_gate_weight.shape[1]
    dma = pltpu.SemaphoreType.DMA
    hbm = pl.BlockSpec(memory_space=pl.ANY)
    near = pl.BlockSpec(memory_space=pltpu.VMEM)
    bf16, f32 = jnp.bfloat16, jnp.float32
    return pl.pallas_call(
        functools.partial(kernel, planes, columns),
        out_shape=jax.ShapeDtypeStruct(tokens.shape, bf16),
        in_specs=[hbm, near, hbm, near, near, hbm, near, hbm, near, near, near, hbm],
        out_specs=hbm,
        scratch_shapes=[
            pltpu.VMEM((PLANE, inner // 128, width, 128), bf16),
            pltpu.VMEM((PLANE, width // 128, inner, 128), bf16),
            pltpu.VMEM((PLANE, 2, blocks, 128, 128), bf16),
            pltpu.VMEM((PLANE, 16, inner), f32),
            pltpu.VMEM((PLANE, length, 128), f32),
            pltpu.VMEM((length, width), bf16),
            pltpu.VMEM((length, width), bf16),
            pltpu.VMEM((planes, length, width), bf16),
            pltpu.VMEM((planes, length, width), bf16),
            pltpu.VMEM((PLANE, 3 * SUB, inner), f32),
            pltpu.VMEM((PLANE, SUB, inner), f32),
            pltpu.VMEM((length // HALVES, width), bf16),
            pltpu.VMEM((length // HALVES, 128), f32),
            pltpu.VMEM((length // HALVES, inner), bf16),
            pltpu.VMEM((4, inner // 2, 128), bf16),
            pltpu.VMEM((2, 4, 128, 128), bf16),
            pltpu.VMEM((4, inner // 2, 128), bf16),
            pltpu.VMEM((2, 4, 128, 128), bf16),
            dma((2, 6, 2)),
            dma((2, 6, 2)),
            dma((3,)),
            dma((2, 3)),
            dma((2, 2)),
            dma((2, 2)),
            dma((3,)),
            dma((2,)),
            dma((4,)),
            dma((2, 3)),
            dma((2, 3)),
            dma,
            dma((planes, HALVES)),
            dma((planes, HALVES)),
            dma((HALVES,)),
            dma((HALVES,)),
            pltpu.SemaphoreType.REGULAR,
            dma((2,)),
            dma((5,)),
            dma((2,)),
            dma((3, 5)),
            dma((2,)),
            dma((5,)),
        ],
        compiler_params=pltpu.CompilerParams(
            collective_id=0, has_side_effects=True, vmem_limit_bytes=60 * 1024 * 1024
        ),
    )(
        tokens,
        layer_norm_scale,
        input_weight,
        filter_weight,
        filter_bias,
        recur_gate_weight,
        recur_gate_bias,
        input_gate_weight,
        input_gate_bias,
        decay_setting,
        spike_log_decay,
        output_weight,
    )


def solution(mesh):
    placed = (
        P("pp", ("fs", "tp"), None, None),
        P("pp", None),
        P("pp", None, None),
        P("pp", None, None),
        P("pp", None),
        P("pp", None, None, None),
        P("pp", None),
        P("pp", None, None, None),
        P("pp", None),
        P("pp", None),
        P("pp", None),
        P("pp", None, None),
    )
    return jax.shard_map(
        local,
        mesh=mesh,
        in_specs=placed,
        out_specs=P("pp", ("fs", "tp"), None, None),
        check_vma=False,
    )
```

```python
import functools

import jax
import jax.numpy as jnp
from jax import lax
from jax.experimental import pallas as pl
from jax.experimental.pallas import tpu as pltpu
from jax.sharding import PartitionSpec as P

PLANE = 4
SUB = 8
HALVES = 1
PARTS = 16
MESH = pl.DeviceIdType.MESH


def prepare(hidden, vec, scaled, power):
    length, width = hidden.shape
    inner = vec.shape[1]
    total = jnp.zeros((length, 128), jnp.float32)
    for n in range(width // 128):
        cols = slice(n * 128, (n + 1) * 128)
        row, start = divmod(n * 128, inner)
        part = hidden[:, cols].astype(jnp.float32)
        total = total + part * part
        scaled[:, cols] = (part * vec[row : row + 1, start : start + 128]).astype(jnp.bfloat16)
    power[...] = total


def layer(hidden, win, wout, gates, vec, following, spike, tail, past, scaled, power, states):
    length, width = hidden.shape
    inner = wout.shape[1]
    steps = length // SUB
    top = lax.broadcasted_iota(jnp.int32, (SUB, 128), 0)

    def project(n):
        weight = jnp.concatenate([win[2 * n], win[2 * n + 1]], axis=1)
        return jnp.dot(scaled[...], weight, preferred_element_type=jnp.float32)

    def conv_of(mixed, block):
        cols = slice(block * 128, (block + 1) * 128)
        mixed = (mixed * scale).reshape(steps, SUB, 128)
        taps = [vec[2 + k : 3 + k, cols] for k in range(4)]
        bias = vec[6:7, cols]
        line = []
        for d in range(3):
            rows = slice(d * SUB, (d + 1) * SUB)
            rolled = pltpu.roll(mixed[steps - 3 + d], 1, 0)
            line.append(jnp.where(top == 0, tail[rows, cols], rolled))
            tail[rows, cols] = rolled
        line += [mixed[t] for t in range(steps)]
        conv = jnp.concatenate(
            [
                (bias + sum(line[t + k] * taps[k] for k in range(4)))[None]
                for t in range(steps)
            ],
            axis=0,
        ).reshape(length, 128)
        weight = jnp.concatenate([gates[0, block], gates[1, block]], axis=1)
        pre = jnp.dot(conv.astype(jnp.bfloat16), weight, preferred_element_type=jnp.float32)
        return conv, pre

    def recur(conv, pre, block):
        cols = slice(block * 128, (block + 1) * 128)
        rate = vec[9:10, cols]
        recall = jnp.tanh(pre[:, :128] + vec[7:8, cols]).reshape(steps, SUB, 128)
        inject = jnp.tanh(pre[:, 128:] + vec[8:9, cols]) + 1.0
        decay = jnp.exp2(recall * rate[None] + (spikes + rate[None]))
        room = jnp.maximum(1.0 - decay * decay, 1e-30)
        update = room * lax.rsqrt(room) * (inject * conv).reshape(steps, SUB, 128)
        sums = [update[0]]
        factors = [decay[0]]
        for t in range(1, steps):
            sums.append(decay[t] * sums[-1] + update[t])
            factors.append(decay[t] * factors[-1])
        first = past[:, cols]
        factor = factors[-1]
        last = sums[-1] + jnp.where(top == 0, factor * first, 0.0)
        for hop in (1, 2, 4):
            last = last + factor * jnp.where(top < hop, 0.0, pltpu.roll(last, hop, 0))
            if hop < 4:
                factor = factor * jnp.where(top < hop, 1.0, pltpu.roll(factor, hop, 0))
        ahead = pltpu.roll(last, 1, 0)
        past[:, cols] = ahead
        carry = jnp.where(top == 0, first, ahead)
        done = jnp.concatenate(
            [(sums[t] + factors[t] * carry)[None] for t in range(steps)], axis=0
        )
        states[:, cols] = done.reshape(length, 128).astype(jnp.bfloat16)

    groups = inner // 256
    first_mixed = project(0)
    scale = lax.rsqrt(jnp.sum(power[...], axis=1, keepdims=True) * (1.0 / width) + 1e-6)
    scale = jnp.broadcast_to(scale, (length, 128))
    spikes = spike[...].reshape(steps, SUB, 128)
    queue = [first_mixed, project(1)]
    for n in range(groups):
        if n + 2 < groups:
            queue.append(project(n + 2))
        left = conv_of(queue[n][:, :128], 2 * n)
        right = conv_of(queue[n][:, 128:], 2 * n + 1)
        recur(*left, 2 * n)
        recur(*right, 2 * n + 1)

    total = jnp.zeros((length, 128), jnp.float32)
    for m in range(width // 256):
        weight = jnp.concatenate([wout[2 * m], wout[2 * m + 1]], axis=1)
        projected = jnp.dot(states[...], weight, preferred_element_type=jnp.float32)
        for half in range(2):
            start = m * 256 + half * 128
            cols = slice(start, start + 128)
            part = hidden[:, cols].astype(jnp.float32) + projected[:, half * 128 : half * 128 + 128]
            hidden[:, cols] = part.astype(jnp.bfloat16)
            total = total + part * part
            row, start = divmod(start, inner)
            scaled[:, cols] = (part * following[row : row + 1, start : start + 128]).astype(
                jnp.bfloat16
            )
    power[...] = total


def reorder(src, dst, back):
    length = src.shape[0]
    steps = length // SUB
    row = lax.broadcasted_iota(jnp.int32, (length, length), 0)
    col = lax.broadcasted_iota(jnp.int32, (length, length), 1)
    if back:
        row, col = col, row
    swap = jnp.where(col == lax.rem(row, SUB) * steps + lax.div(row, SUB), 1.0, 0.0)
    swap = swap.astype(jnp.bfloat16)
    for n in range(src.shape[1] // 256):
        cols = slice(n * 256, (n + 1) * 256)
        moved = jnp.dot(swap, src[:, cols], preferred_element_type=jnp.float32)
        dst[:, cols] = moved.astype(jnp.bfloat16)


def kernel(
    planes, columns,
    tok, gain, win, taps, conv_bias, recur_gate, recur_bias, input_gate, input_bias, setting,
    spikes, wout, out,
    win_all, wout_all, gates_all, vec_all, spike_all, raw, home, act, final, tails, pasts,
    scaled, power, states, relay_wout, relay_gate,
    onward_wout, onward_gate,
    y_recv, x_recv, d_recv, g_recv, y_send, x_send, d_send, g_send, own_sem,
    small_recv, small_send, raw_sem, act_recv, act_send, home_sem, out_recv, lag_sem,
    f_send, f_recv, h_send, h_recv, k_send, k_recv,
):
    position = lax.axis_index("pp")
    x = lax.axis_index("fs")
    core = lax.axis_index("tp")
    z = position // PLANE
    y = lax.rem(position, PLANE)
    parity = lax.rem(x, 2)
    length, width = raw.shape
    inner = wout_all.shape[2]
    chunk = length // HALVES

    def at_y(by):
        return z * PLANE + lax.rem(y + by, PLANE)

    def plane_slot(by):
        return lax.rem(y + by, PLANE)

    def rows_of(half):
        return pl.ds(pl.multiple_of(half * chunk, chunk), chunk)

    up, down, across = {"pp": at_y(1)}, {"pp": at_y(3)}, {"pp": at_y(2)}
    right, left = {"fs": lax.rem(x + 1, columns)}, {"fs": lax.rem(x + columns - 1, columns)}
    sibling = {"tp": 1 - core}
    z_peers = [{"pp": lax.rem(z + by, planes) * PLANE + y} for by in range(1, planes)]

    own = [
        pltpu.make_async_copy(source.at[0], gates_all.at[y, n], own_sem.at[n])
        for n, source in enumerate((recur_gate, input_gate))
    ]
    for copy in own:
        copy.start()
    pltpu.make_async_copy(tok.at[0, 0], raw, raw_sem).start()

    barrier = pltpu.get_barrier_semaphore()
    mirror = [{"pp": (planes - 1 - z) * PLANE + lax.rem(y + by, PLANE)} for by in range(1, 4)]
    peers = [up, down, across, right, left, sibling] + z_peers + mirror
    for peer in peers:
        pl.semaphore_signal(barrier, inc=1, device_id=peer, device_id_type=MESH)

    vec_all[y, 0:1] = gain[:, :inner]
    vec_all[y, 1:2] = gain[:, inner:]
    log2e = 1.4426950408889634
    vec_all[y, 2:6] = 0.5 * taps[0]
    vec_all[y, 6:7] = 0.5 * conv_bias[...]
    vec_all[y, 7:8] = 0.5 * recur_bias[...]
    vec_all[y, 8:9] = 0.5 * input_bias[...]
    below = -setting[...]
    softplus = jnp.maximum(below, 0.0) + jnp.log1p(jnp.exp(-jnp.abs(below)))
    vec_all[y, 9:10] = (-4.0 * log2e) * softplus
    row = lax.broadcasted_iota(jnp.int32, (length, length), 0)
    col = lax.broadcasted_iota(jnp.int32, (length, length), 1)
    within = lax.rem(row, chunk)
    token = (row - within) + lax.rem(within, SUB) * (chunk // SUB) + lax.div(within, SUB)
    picked = jnp.sum(jnp.where(col == token, spikes[...], 0.0), axis=1, keepdims=True)
    spike_all[y] = jnp.broadcast_to(picked * log2e, (length, 128))

    pl.semaphore_wait(barrier, len(peers))

    gathered = (win_all, wout_all)

    def piece(a, slot, index):
        if a == 1:
            return wout_all.at[slot, index]
        half = win_all.shape[2] // 2
        return win_all.at[slot, index // 2, pl.ds(pl.multiple_of(lax.rem(index, 2) * half, half), half)]

    def source(a, index):
        if a == 1:
            return wout.at[0, :, pl.ds(pl.multiple_of(index * 128, 128), 128)]
        half = win_all.shape[2] // 2
        return win.at[
            0,
            pl.ds(pl.multiple_of(lax.rem(index, 2) * half, half), half),
            pl.ds(pl.multiple_of(index // 2 * 128, 128), 128),
        ]

    def gate_piece(slot, index):
        return gates_all.at[slot, :, pl.ds(4 * core + 2 * index, 2)]

    def push(src, dst, send_sem, recv_sem, to):
        pltpu.make_async_remote_copy(
            src_ref=src, dst_ref=dst, send_sem=send_sem, recv_sem=recv_sem,
            device_id=to, device_id_type=MESH,
        ).start()

    def send(a, src, slot, index, send_sem, recv_sem, to):
        push(src, piece(a, slot, index), send_sem, recv_sem, to)

    def await_bytes(ref, sem):
        pltpu.make_async_copy(ref, ref, sem).wait()

    def pieces_of(a, count):
        tiles = count // 2 if a == 0 else count
        if count == 6:
            return gathered[a].at[0, pl.ds(0, tiles)]
        return gathered[a].at[pl.ds(0, 2), pl.ds(0, tiles // 2)]

    mine = 8 * parity + 4 * core
    other = 8 * (1 - parity) + 4 * core

    first, last = z == 0, z == planes - 1
    lower = pl.ds(wout_all.shape[2] // 2, wout_all.shape[2] // 2)
    upper = pl.ds(0, wout_all.shape[2] // 2)
    detours = [(8 * side + 4 * core + j) for side in range(2) for j in (1, 3)]
    core_gates = pl.ds(4 * core, 4)

    for copy in own:
        copy.wait()

    @pl.when(first)
    def _():
        to = {"pp": (planes - 1) * PLANE + y}
        for n, index in enumerate(detours):
            column = pl.ds(pl.multiple_of(index * 128, 128), 128)
            push(wout.at[0, lower, column], relay_wout.at[n], f_send.at[0], f_recv.at[n], to)
        push(gates_all.at[y, :, core_gates], relay_gate, f_send.at[1], f_recv.at[4], to)

    def split(a, j, act_on):
        if a == 0 or j % 2 == 0:
            act_on(lambda ref: ref)
            return

        @pl.when(first)
        def _():
            act_on(lambda ref: ref.at[upper])

        @pl.when(z != 0)
        def _():
            act_on(lambda ref: ref)

    def start_unit(unit):
        for a in range(2):
            for side, to in enumerate((up, down)):
                j = (unit + 2 * side) % 4
                split(a, j, lambda cut: push(
                    cut(source(a, mine + j)), cut(piece(a, y, mine + j)),
                    y_send.at[side, a], y_recv.at[side, unit, a], to))

    start_unit(0)

    def detour(slot, n):
        return wout_all.at[slot, detours[n], lower] if n < 4 else gates_all.at[slot, :, core_gates]

    headings = (3, 1, 1, 1, 3)

    @pl.when(last)
    def _():
        for n, heading in enumerate(headings):
            ref, store = (relay_wout.at[n], onward_wout.at[n]) if n < 4 else (relay_gate, onward_gate)
            await_bytes(ref, f_recv.at[n])
            push(ref, store, k_send.at[n // 4], k_recv.at[n], {"pp": at_y(heading)})
            by = 4 - heading
            push(ref, detour(y, n), h_send.at[n // 4], h_recv.at[by - 1, n],
                 {"pp": lax.rem(y + by, PLANE)})

    start_unit(1)

    @pl.when(last)
    def _():
        for n, heading in enumerate(headings):
            ref = onward_wout.at[n] if n < 4 else onward_gate
            await_bytes(ref, k_recv.at[n])
            dst = detour(plane_slot(4 - heading), n)
            push(ref, dst, h_send.at[n // 4], h_recv.at[1, n],
                 {"pp": lax.rem(y + heading, PLANE)})
            push(ref, dst, h_send.at[n // 4], h_recv.at[heading - 1, n], {"pp": y})

    start_unit(2)
    start_unit(3)
    smalls = (vec_all, spike_all)
    for n, ref in enumerate(smalls):
        for by in range(1, 4):
            pltpu.make_async_remote_copy(
                src_ref=ref.at[y], dst_ref=ref.at[y], send_sem=small_send.at[n, by - 1],
                recv_sem=small_recv.at[n, by - 1],
                device_id={"pp": at_y(by)}, device_id_type=MESH,
            ).start()
    for n in range(win_all.shape[1]):
        pltpu.make_async_copy(
            win.at[0, :, n * 128 : (n + 1) * 128], win_all.at[y, n], own_sem.at[2]
        ).start()
    for n in range(wout_all.shape[1]):
        pltpu.make_async_copy(
            wout.at[0, :, n * 128 : (n + 1) * 128], wout_all.at[y, n], own_sem.at[3]
        ).start()

    await_bytes(raw, raw_sem)
    for half in range(HALVES):
        rows = slice(half * chunk, (half + 1) * chunk)
        reorder(raw.at[rows], home.at[rows], False)

        @pl.when(z == 0)
        def _():
            pltpu.make_async_copy(home.at[rows], act.at[0, rows], act_recv.at[0, half]).start()

    def send_home():
        for half in range(HALVES):
            rows = slice(half * chunk, (half + 1) * chunk)
            push(home.at[rows], act.at[z, rows], home_sem.at[half], act_recv.at[z, half], {"pp": y})

    pl.when((z == 1) | last)(send_home)

    def arrivals(unit):
        from_below = (plane_slot(3), unit) if unit < 4 else (plane_slot(2), unit - 4)
        from_above = (plane_slot(1), (unit + 2) % 4) if unit < 4 else (plane_slot(2), unit - 2)
        return from_below, from_above

    x_units = []
    for unit in range(6):
        below, above = arrivals(unit)
        x_units.append((below, above) if below[1] < 2 else (above, below))

    def relay_y(unit, a):
        for side, (slot, j) in enumerate(arrivals(unit)):
            def forward(cut):
                ref = cut(piece(a, slot, mine + j))
                await_bytes(ref, y_recv.at[side, unit, a])
                if unit < 2:
                    push(ref, ref, y_send.at[side, a], y_recv.at[side, 4 + unit, a],
                         up if side == 0 else down)
                x_side = 0 if j < 2 else 1
                push(ref, ref, x_send.at[x_side, a], x_recv.at[x_side, unit, a],
                     left if x_side == 0 else right)
                push(ref, ref, d_send.at[a], d_recv.at[a], sibling)

            split(a, j, forward)

    def relay_x(unit, a):
        for side, (slot, j) in enumerate(x_units[unit]):
            def forward(cut):
                ref = cut(piece(a, slot, other + j))
                await_bytes(ref, x_recv.at[side, unit, a])
                push(ref, ref, d_send.at[a], d_recv.at[a], sibling)

            split(a, j, forward)

    def relay_gates(n):
        slots = ((3, 0), (3, 1), (2, 0)), ((1, 1), (1, 0), (2, 1))
        for side in range(2):
            by, index = slots[side][n]
            ref = gate_piece(plane_slot(by), index)
            await_bytes(ref, g_recv.at[side, n])
            if n == 0:
                push(ref, ref, g_send.at[side], g_recv.at[side, 2], up if side == 0 else down)
            push(ref, ref, d_send.at[2], d_recv.at[2], sibling)

    for unit in range(6):
        for a in range(2):
            relay_y(unit, a)
            if unit > 0:
                relay_x(unit - 1, a)
        if unit == 4:
            pl.when((z > 1) & (z != planes - 1))(send_home)
        if unit == 1:
            @pl.when(z != 0)
            def _():
                for n in range(2):
                    for side, to in enumerate((up, down)):
                        ref = gate_piece(y, n if side == 0 else 1 - n)
                        push(ref, ref, g_send.at[side], g_recv.at[side, n], to)

    @pl.when(z != 0)
    def _():
        for n in range(3):
            relay_gates(n)

    @pl.when(first)
    def _():
        for n in range(5):
            for by in range(1, 4):
                slot = plane_slot(4 - by)
                ref = detour(slot, n)
                await_bytes(ref, h_recv.at[by - 1, n])
                push(ref, ref, d_send.at[1 + n // 4], d_recv.at[1 + n // 4], sibling)

    for a in range(2):
        relay_x(5, a)

    await_bytes(win_all.at[y], own_sem.at[2])
    await_bytes(wout_all.at[y], own_sem.at[3])
    for n, ref in enumerate(smalls):
        for by in range(1, 4):
            await_bytes(ref.at[plane_slot(4 - by)], small_recv.at[n, by - 1])
    for a in range(2):
        await_bytes(pieces_of(a, 24), d_recv.at[a])
    await_bytes(gates_all.at[pl.ds(0, 3), :, pl.ds(0, 4)], d_recv.at[2])

    def micro(step, token):
        i = step // HALVES
        half = lax.rem(step, HALVES)
        rows = rows_of(half)
        here = act.at[i, rows]
        await_bytes(here, act_recv.at[i, half])

        @pl.when(half == 0)
        def _():
            tails[...] = jnp.zeros_like(tails)
            pasts[...] = jnp.zeros_like(pasts)

        @pl.when((z == 0) & (core == 1) & (step == 0))
        def _():
            pl.semaphore_wait(lag_sem, 1)

        prepare(here, vec_all.at[0], scaled, power)

        def one(s, token):
            layer(here, win_all.at[s], wout_all.at[s], gates_all.at[s], vec_all.at[s],
                  vec_all.at[lax.rem(s + 1, PLANE)], spike_all.at[s, rows], tails.at[s],
                  pasts.at[s], scaled, power, states)

            @pl.when((z == 0) & (core == 0) & (step == 0) & (s == 2))
            def _():
                pl.semaphore_signal(lag_sem, inc=1, device_id=sibling, device_id_type=MESH)

            return token

        lax.fori_loop(0, PLANE, one, 0)

        @pl.when(z < planes - 1)
        def _():
            pltpu.make_async_remote_copy(
                src_ref=here, dst_ref=here, send_sem=act_send.at[i, half],
                recv_sem=act_recv.at[i, half],
                device_id={"pp": lax.rem(z + 1, planes) * PLANE + y}, device_id_type=MESH,
            ).start()

        @pl.when(z == planes - 1)
        def _():
            reorder(here, final.at[i, rows], True)

            @pl.when(i < planes - 1)
            def _():
                pltpu.make_async_remote_copy(
                    src_ref=final.at[i, rows], dst_ref=out.at[0, 0, rows],
                    send_sem=act_send.at[i, half], recv_sem=out_recv.at[half],
                    device_id={"pp": i * PLANE + y}, device_id_type=MESH,
                ).start()

            @pl.when(i == planes - 1)
            def _():
                pltpu.make_async_copy(
                    final.at[i, rows], out.at[0, 0, rows], out_recv.at[half]
                ).start()

        return token

    lax.fori_loop(0, planes * HALVES, micro, 0)

    for half in range(HALVES):
        rows = slice(half * chunk, (half + 1) * chunk)
        await_bytes(out.at[0, 0, rows], out_recv.at[half])
        for i in range(planes):
            if i < planes - 1:
                await_bytes(act.at[i, rows], act_send.at[i, half])
            else:
                @pl.when(z < planes - 1)
                def _():
                    await_bytes(act.at[i, rows], act_send.at[i, half])

        @pl.when(z != 0)
        def _():
            await_bytes(home.at[rows], home_sem.at[half])

    for n, ref in enumerate(smalls):
        for by in range(1, 4):
            await_bytes(ref.at[y], small_send.at[n, by - 1])
    for side in range(2):
        for sem in (y_send, x_send):
            await_bytes(pieces_of(0, 6), sem.at[side, 0])

            @pl.when(first)
            def _():
                await_bytes(wout_all.at[0, pl.ds(0, 9), upper], sem.at[side, 1])

            @pl.when(z != 0)
            def _():
                await_bytes(pieces_of(1, 6), sem.at[side, 1])

        @pl.when(z != 0)
        def _():
            await_bytes(gates_all.at[pl.ds(0, 3), :, pl.ds(0, 2)], g_send.at[side])

    @pl.when(first)
    def _():
        await_bytes(relay_wout, f_send.at[0])
        await_bytes(relay_gate, f_send.at[1])

    @pl.when(last)
    def _():
        await_bytes(onward_wout, k_send.at[0])
        await_bytes(onward_gate, k_send.at[1])
        await_bytes(wout_all.at[0, pl.ds(0, 12), upper], h_send.at[0])
        await_bytes(gates_all.at[pl.ds(0, 3), :, pl.ds(0, 4)], h_send.at[1])

    for a in range(2):
        await_bytes(pieces_of(a, 24), d_send.at[a])
    await_bytes(gates_all.at[pl.ds(0, 3), :, pl.ds(0, 4)], d_send.at[2])


def local(
    tokens,
    layer_norm_scale,
    input_weight,
    filter_weight,
    filter_bias,
    recur_gate_weight,
    recur_gate_bias,
    input_gate_weight,
    input_gate_bias,
    decay_setting,
    spike_log_decay,
    output_weight,
):
    planes = lax.axis_size("pp") // PLANE
    columns = lax.axis_size("fs")
    length, width = tokens.shape[2:]
    inner = input_weight.shape[2]
    blocks = recur_gate_weight.shape[1]
    dma = pltpu.SemaphoreType.DMA
    hbm = pl.BlockSpec(memory_space=pl.ANY)
    near = pl.BlockSpec(memory_space=pltpu.VMEM)
    bf16, f32 = jnp.bfloat16, jnp.float32
    return pl.pallas_call(
        functools.partial(kernel, planes, columns),
        out_shape=jax.ShapeDtypeStruct(tokens.shape, bf16),
        in_specs=[hbm, near, hbm, near, near, hbm, near, hbm, near, near, near, hbm],
        out_specs=near,
        scratch_shapes=[
            pltpu.VMEM((PLANE, inner // 128, width, 128), bf16),
            pltpu.VMEM((PLANE, width // 128, inner, 128), bf16),
            pltpu.VMEM((PLANE, 2, blocks, 128, 128), bf16),
            pltpu.VMEM((PLANE, 16, inner), f32),
            pltpu.VMEM((PLANE, length, 128), f32),
            pltpu.VMEM((length, width), bf16),
            pltpu.VMEM((length, width), bf16),
            pltpu.VMEM((planes, length, width), bf16),
            pltpu.VMEM((planes, length, width), bf16),
            pltpu.VMEM((PLANE, 3 * SUB, inner), f32),
            pltpu.VMEM((PLANE, SUB, inner), f32),
            pltpu.VMEM((length // HALVES, width), bf16),
            pltpu.VMEM((length // HALVES, 128), f32),
            pltpu.VMEM((length // HALVES, inner), bf16),
            pltpu.VMEM((4, inner // 2, 128), bf16),
            pltpu.VMEM((2, 4, 128, 128), bf16),
            pltpu.VMEM((4, inner // 2, 128), bf16),
            pltpu.VMEM((2, 4, 128, 128), bf16),
            dma((2, 6, 2)),
            dma((2, 6, 2)),
            dma((3,)),
            dma((2, 3)),
            dma((2, 2)),
            dma((2, 2)),
            dma((3,)),
            dma((2,)),
            dma((4,)),
            dma((2, 3)),
            dma((2, 3)),
            dma,
            dma((planes, HALVES)),
            dma((planes, HALVES)),
            dma((HALVES,)),
            dma((HALVES,)),
            pltpu.SemaphoreType.REGULAR,
            dma((2,)),
            dma((5,)),
            dma((2,)),
            dma((3, 5)),
            dma((2,)),
            dma((5,)),
        ],
        compiler_params=pltpu.CompilerParams(
            collective_id=0, has_side_effects=True, vmem_limit_bytes=60 * 1024 * 1024
        ),
    )(
        tokens,
        layer_norm_scale,
        input_weight,
        filter_weight,
        filter_bias,
        recur_gate_weight,
        recur_gate_bias,
        input_gate_weight,
        input_gate_bias,
        decay_setting,
        spike_log_decay,
        output_weight,
    )


def solution(mesh):
    placed = (
        P("pp", ("fs", "tp"), None, None),
        P("pp", None),
        P("pp", None, None),
        P("pp", None, None),
        P("pp", None),
        P("pp", None, None, None),
        P("pp", None),
        P("pp", None, None, None),
        P("pp", None),
        P("pp", None),
        P("pp", None),
        P("pp", None, None),
    )
    return jax.shard_map(
        local,
        mesh=mesh,
        in_specs=placed,
        out_specs=P("pp", ("fs", "tp"), None, None),
        check_vma=False,
    )
```

```python
import functools

import jax
import jax.numpy as jnp
from jax import lax
from jax.experimental import pallas as pl
from jax.experimental.pallas import tpu as pltpu
from jax.sharding import PartitionSpec as P

PLANE = 4
SUB = 8
HALVES = 1
PARTS = 16
MESH = pl.DeviceIdType.MESH


def prepare(hidden, vec, scaled, power):
    length, width = hidden.shape
    inner = vec.shape[1]
    total = jnp.zeros((length, 128), jnp.float32)
    for n in range(width // 128):
        cols = slice(n * 128, (n + 1) * 128)
        row, start = divmod(n * 128, inner)
        part = hidden[:, cols].astype(jnp.float32)
        total = total + part * part
        scaled[:, cols] = (part * vec[row : row + 1, start : start + 128]).astype(jnp.bfloat16)
    power[...] = total


def layer(hidden, win, wout, gates, vec, following, spike, tail, past, scaled, power, states):
    length, width = hidden.shape
    inner = wout.shape[1]
    steps = length // SUB
    top = lax.broadcasted_iota(jnp.int32, (SUB, 128), 0)

    def project(n):
        weight = jnp.concatenate([win[2 * n], win[2 * n + 1]], axis=1)
        return jnp.dot(scaled[...], weight, preferred_element_type=jnp.float32)

    def conv_of(mixed, block):
        cols = slice(block * 128, (block + 1) * 128)
        mixed = (mixed * scale).reshape(steps, SUB, 128)
        taps = [vec[2 + k : 3 + k, cols] for k in range(4)]
        bias = vec[6:7, cols]
        line = []
        for d in range(3):
            rows = slice(d * SUB, (d + 1) * SUB)
            rolled = pltpu.roll(mixed[steps - 3 + d], 1, 0)
            line.append(jnp.where(top == 0, tail[rows, cols], rolled))
            tail[rows, cols] = rolled
        line += [mixed[t] for t in range(steps)]
        conv = jnp.concatenate(
            [
                (bias + sum(line[t + k] * taps[k] for k in range(4)))[None]
                for t in range(steps)
            ],
            axis=0,
        ).reshape(length, 128)
        weight = jnp.concatenate([gates[0, block], gates[1, block]], axis=1)
        pre = jnp.dot(conv.astype(jnp.bfloat16), weight, preferred_element_type=jnp.float32)
        return conv, pre

    def recur(conv, pre, block):
        cols = slice(block * 128, (block + 1) * 128)
        rate = vec[9:10, cols]
        recall = jnp.tanh(pre[:, :128] + vec[7:8, cols]).reshape(steps, SUB, 128)
        inject = jnp.tanh(pre[:, 128:] + vec[8:9, cols]) + 1.0
        decay = jnp.exp2(recall * rate[None] + (spikes + rate[None]))
        room = jnp.maximum(1.0 - decay * decay, 1e-30)
        update = room * lax.rsqrt(room) * (inject * conv).reshape(steps, SUB, 128)
        sums = [update[0]]
        factors = [decay[0]]
        for t in range(1, steps):
            sums.append(decay[t] * sums[-1] + update[t])
            factors.append(decay[t] * factors[-1])
        first = past[:, cols]
        factor = factors[-1]
        last = sums[-1] + jnp.where(top == 0, factor * first, 0.0)
        for hop in (1, 2, 4):
            last = last + factor * jnp.where(top < hop, 0.0, pltpu.roll(last, hop, 0))
            if hop < 4:
                factor = factor * jnp.where(top < hop, 1.0, pltpu.roll(factor, hop, 0))
        ahead = pltpu.roll(last, 1, 0)
        past[:, cols] = ahead
        carry = jnp.where(top == 0, first, ahead)
        done = jnp.concatenate(
            [(sums[t] + factors[t] * carry)[None] for t in range(steps)], axis=0
        )
        states[:, cols] = done.reshape(length, 128).astype(jnp.bfloat16)

    groups = inner // 256
    first_mixed = project(0)
    scale = lax.rsqrt(jnp.sum(power[...], axis=1, keepdims=True) * (1.0 / width) + 1e-6)
    scale = jnp.broadcast_to(scale, (length, 128))
    spikes = spike[...].reshape(steps, SUB, 128)
    queue = [first_mixed, project(1)]
    for n in range(groups):
        if n + 2 < groups:
            queue.append(project(n + 2))
        left = conv_of(queue[n][:, :128], 2 * n)
        right = conv_of(queue[n][:, 128:], 2 * n + 1)
        recur(*left, 2 * n)
        recur(*right, 2 * n + 1)

    total = jnp.zeros((length, 128), jnp.float32)
    for m in range(width // 256):
        weight = jnp.concatenate([wout[2 * m], wout[2 * m + 1]], axis=1)
        projected = jnp.dot(states[...], weight, preferred_element_type=jnp.float32)
        for half in range(2):
            start = m * 256 + half * 128
            cols = slice(start, start + 128)
            part = hidden[:, cols].astype(jnp.float32) + projected[:, half * 128 : half * 128 + 128]
            hidden[:, cols] = part.astype(jnp.bfloat16)
            total = total + part * part
            row, start = divmod(start, inner)
            scaled[:, cols] = (part * following[row : row + 1, start : start + 128]).astype(
                jnp.bfloat16
            )
    power[...] = total


def reorder(src, dst, back):
    length = src.shape[0]
    steps = length // SUB
    row = lax.broadcasted_iota(jnp.int32, (length, length), 0)
    col = lax.broadcasted_iota(jnp.int32, (length, length), 1)
    if back:
        row, col = col, row
    swap = jnp.where(col == lax.rem(row, SUB) * steps + lax.div(row, SUB), 1.0, 0.0)
    swap = swap.astype(jnp.bfloat16)
    for n in range(src.shape[1] // 256):
        cols = slice(n * 256, (n + 1) * 256)
        moved = jnp.dot(swap, src[:, cols], preferred_element_type=jnp.float32)
        dst[:, cols] = moved.astype(jnp.bfloat16)


def kernel(
    planes, columns,
    tok, gain, win, taps, conv_bias, recur_gate, recur_bias, input_gate, input_bias, setting,
    spikes, wout, out,
    win_all, wout_all, gates_all, vec_all, spike_all, raw, home, act, final, tails, pasts,
    scaled, power, states, relay_wout, relay_gate,
    onward_wout, onward_gate,
    y_recv, x_recv, d_recv, g_recv, y_send, x_send, d_send, g_send, own_sem,
    small_recv, small_send, raw_sem, act_recv, act_send, home_sem, out_recv, lag_sem,
    f_send, f_recv, h_send, h_recv, k_send, k_recv,
):
    position = lax.axis_index("pp")
    x = lax.axis_index("fs")
    core = lax.axis_index("tp")
    z = position // PLANE
    y = lax.rem(position, PLANE)
    parity = lax.rem(x, 2)
    length, width = raw.shape
    inner = wout_all.shape[2]
    chunk = length // HALVES

    def at_y(by):
        return z * PLANE + lax.rem(y + by, PLANE)

    def plane_slot(by):
        return lax.rem(y + by, PLANE)

    def rows_of(half):
        return pl.ds(pl.multiple_of(half * chunk, chunk), chunk)

    up, down, across = {"pp": at_y(1)}, {"pp": at_y(3)}, {"pp": at_y(2)}
    right, left = {"fs": lax.rem(x + 1, columns)}, {"fs": lax.rem(x + columns - 1, columns)}
    sibling = {"tp": 1 - core}
    z_peers = [{"pp": lax.rem(z + by, planes) * PLANE + y} for by in range(1, planes)]

    own = [
        pltpu.make_async_copy(source.at[0], gates_all.at[y, n], own_sem.at[n])
        for n, source in enumerate((recur_gate, input_gate))
    ]
    for copy in own:
        copy.start()
    pltpu.make_async_copy(tok.at[0, 0], raw, raw_sem).start()

    barrier = pltpu.get_barrier_semaphore()
    mirror = [{"pp": (planes - 1 - z) * PLANE + lax.rem(y + by, PLANE)} for by in range(1, 4)]
    peers = [up, down, across, right, left, sibling] + z_peers + mirror
    for peer in peers:
        pl.semaphore_signal(barrier, inc=1, device_id=peer, device_id_type=MESH)

    vec_all[y, 0:1] = gain[:, :inner]
    vec_all[y, 1:2] = gain[:, inner:]
    log2e = 1.4426950408889634
    vec_all[y, 2:6] = 0.5 * taps[0]
    vec_all[y, 6:7] = 0.5 * conv_bias[...]
    vec_all[y, 7:8] = 0.5 * recur_bias[...]
    vec_all[y, 8:9] = 0.5 * input_bias[...]
    below = -setting[...]
    softplus = jnp.maximum(below, 0.0) + jnp.log1p(jnp.exp(-jnp.abs(below)))
    vec_all[y, 9:10] = (-4.0 * log2e) * softplus
    row = lax.broadcasted_iota(jnp.int32, (length, length), 0)
    col = lax.broadcasted_iota(jnp.int32, (length, length), 1)
    within = lax.rem(row, chunk)
    token = (row - within) + lax.rem(within, SUB) * (chunk // SUB) + lax.div(within, SUB)
    picked = jnp.sum(jnp.where(col == token, spikes[...], 0.0), axis=1, keepdims=True)
    spike_all[y] = jnp.broadcast_to(picked * log2e, (length, 128))

    pl.semaphore_wait(barrier, len(peers))

    gathered = (win_all, wout_all)

    def piece(a, slot, index):
        if a == 1:
            return wout_all.at[slot, index]
        half = win_all.shape[2] // 2
        return win_all.at[slot, index // 2, pl.ds(pl.multiple_of(lax.rem(index, 2) * half, half), half)]

    def source(a, index):
        if a == 1:
            return wout.at[0, :, pl.ds(pl.multiple_of(index * 128, 128), 128)]
        half = win_all.shape[2] // 2
        return win.at[
            0,
            pl.ds(pl.multiple_of(lax.rem(index, 2) * half, half), half),
            pl.ds(pl.multiple_of(index // 2 * 128, 128), 128),
        ]

    def gate_piece(slot, index):
        return gates_all.at[slot, :, pl.ds(4 * core + 2 * index, 2)]

    def push(src, dst, send_sem, recv_sem, to):
        pltpu.make_async_remote_copy(
            src_ref=src, dst_ref=dst, send_sem=send_sem, recv_sem=recv_sem,
            device_id=to, device_id_type=MESH,
        ).start()

    def send(a, src, slot, index, send_sem, recv_sem, to):
        push(src, piece(a, slot, index), send_sem, recv_sem, to)

    def await_bytes(ref, sem):
        pltpu.make_async_copy(ref, ref, sem).wait()

    def pieces_of(a, count):
        tiles = count // 2 if a == 0 else count
        if count == 6:
            return gathered[a].at[0, pl.ds(0, tiles)]
        return gathered[a].at[pl.ds(0, 2), pl.ds(0, tiles // 2)]

    mine = 8 * parity + 4 * core
    other = 8 * (1 - parity) + 4 * core

    first, last = z == 0, z == planes - 1
    lower = pl.ds(wout_all.shape[2] // 2, wout_all.shape[2] // 2)
    upper = pl.ds(0, wout_all.shape[2] // 2)
    detours = [(8 * side + 4 * core + j) for side in range(2) for j in (1, 3)]
    core_gates = pl.ds(4 * core, 4)

    @pl.when(first)
    def _():
        to = {"pp": (planes - 1) * PLANE + y}
        for n, index in enumerate(detours):
            column = pl.ds(pl.multiple_of(index * 128, 128), 128)
            push(wout.at[0, lower, column], relay_wout.at[n], f_send.at[0], f_recv.at[n], to)

    def split(a, j, act_on):
        if a == 0 or j % 2 == 0:
            act_on(lambda ref: ref)
            return

        @pl.when(first)
        def _():
            act_on(lambda ref: ref.at[upper])

        @pl.when(z != 0)
        def _():
            act_on(lambda ref: ref)

    def start_unit(unit):
        for a in range(2):
            for side, to in enumerate((up, down)):
                j = (unit + 2 * side) % 4
                split(a, j, lambda cut: push(
                    cut(source(a, mine + j)), cut(piece(a, y, mine + j)),
                    y_send.at[side, a], y_recv.at[side, unit, a], to))

    start_unit(0)

    for copy in own:
        copy.wait()

    @pl.when(first)
    def _():
        to = {"pp": (planes - 1) * PLANE + y}
        push(gates_all.at[y, :, core_gates], relay_gate, f_send.at[1], f_recv.at[4], to)

    def detour(slot, n):
        return wout_all.at[slot, detours[n], lower] if n < 4 else gates_all.at[slot, :, core_gates]

    headings = (3, 1, 1, 1, 3)

    @pl.when(last)
    def _():
        for n, heading in enumerate(headings):
            ref, store = (relay_wout.at[n], onward_wout.at[n]) if n < 4 else (relay_gate, onward_gate)
            await_bytes(ref, f_recv.at[n])
            push(ref, store, k_send.at[n // 4], k_recv.at[n], {"pp": at_y(heading)})
            by = 4 - heading
            push(ref, detour(y, n), h_send.at[n // 4], h_recv.at[by - 1, n],
                 {"pp": lax.rem(y + by, PLANE)})

    start_unit(1)

    @pl.when(last)
    def _():
        for n, heading in enumerate(headings):
            ref = onward_wout.at[n] if n < 4 else onward_gate
            await_bytes(ref, k_recv.at[n])
            dst = detour(plane_slot(4 - heading), n)
            push(ref, dst, h_send.at[n // 4], h_recv.at[1, n],
                 {"pp": lax.rem(y + heading, PLANE)})
            push(ref, dst, h_send.at[n // 4], h_recv.at[heading - 1, n], {"pp": y})

    start_unit(2)
    start_unit(3)
    smalls = (vec_all, spike_all)
    for n, ref in enumerate(smalls):
        for by in range(1, 4):
            pltpu.make_async_remote_copy(
                src_ref=ref.at[y], dst_ref=ref.at[y], send_sem=small_send.at[n, by - 1],
                recv_sem=small_recv.at[n, by - 1],
                device_id={"pp": at_y(by)}, device_id_type=MESH,
            ).start()
    for n in range(win_all.shape[1]):
        pltpu.make_async_copy(
            win.at[0, :, n * 128 : (n + 1) * 128], win_all.at[y, n], own_sem.at[2]
        ).start()
    for n in range(wout_all.shape[1]):
        pltpu.make_async_copy(
            wout.at[0, :, n * 128 : (n + 1) * 128], wout_all.at[y, n], own_sem.at[3]
        ).start()

    await_bytes(raw, raw_sem)
    for half in range(HALVES):
        rows = slice(half * chunk, (half + 1) * chunk)
        reorder(raw.at[rows], home.at[rows], False)

        @pl.when(z == 0)
        def _():
            pltpu.make_async_copy(home.at[rows], act.at[0, rows], act_recv.at[0, half]).start()

    def send_home():
        for half in range(HALVES):
            rows = slice(half * chunk, (half + 1) * chunk)
            push(home.at[rows], act.at[z, rows], home_sem.at[half], act_recv.at[z, half], {"pp": y})

    pl.when((z == 1) | last)(send_home)

    def arrivals(unit):
        from_below = (plane_slot(3), unit) if unit < 4 else (plane_slot(2), unit - 4)
        from_above = (plane_slot(1), (unit + 2) % 4) if unit < 4 else (plane_slot(2), unit - 2)
        return from_below, from_above

    x_units = []
    for unit in range(6):
        below, above = arrivals(unit)
        x_units.append((below, above) if below[1] < 2 else (above, below))

    def relay_y(unit, a):
        for side, (slot, j) in enumerate(arrivals(unit)):
            def forward(cut):
                ref = cut(piece(a, slot, mine + j))
                await_bytes(ref, y_recv.at[side, unit, a])
                if unit < 2:
                    push(ref, ref, y_send.at[side, a], y_recv.at[side, 4 + unit, a],
                         up if side == 0 else down)
                x_side = 0 if j < 2 else 1
                push(ref, ref, x_send.at[x_side, a], x_recv.at[x_side, unit, a],
                     left if x_side == 0 else right)
                push(ref, ref, d_send.at[a], d_recv.at[a], sibling)

            split(a, j, forward)

    def relay_x(unit, a):
        for side, (slot, j) in enumerate(x_units[unit]):
            def forward(cut):
                ref = cut(piece(a, slot, other + j))
                await_bytes(ref, x_recv.at[side, unit, a])
                push(ref, ref, d_send.at[a], d_recv.at[a], sibling)

            split(a, j, forward)

    def relay_gates(n):
        slots = ((3, 0), (3, 1), (2, 0)), ((1, 1), (1, 0), (2, 1))
        for side in range(2):
            by, index = slots[side][n]
            ref = gate_piece(plane_slot(by), index)
            await_bytes(ref, g_recv.at[side, n])
            if n == 0:
                push(ref, ref, g_send.at[side], g_recv.at[side, 2], up if side == 0 else down)
            push(ref, ref, d_send.at[2], d_recv.at[2], sibling)

    for unit in range(6):
        for a in range(2):
            relay_y(unit, a)
            if unit > 0:
                relay_x(unit - 1, a)
        if unit == 4:
            pl.when((z > 1) & (z != planes - 1))(send_home)
        if unit == 1:
            @pl.when(z != 0)
            def _():
                for n in range(2):
                    for side, to in enumerate((up, down)):
                        ref = gate_piece(y, n if side == 0 else 1 - n)
                        push(ref, ref, g_send.at[side], g_recv.at[side, n], to)

    @pl.when(z != 0)
    def _():
        for n in range(3):
            relay_gates(n)

    @pl.when(first)
    def _():
        for n in range(5):
            for by in range(1, 4):
                slot = plane_slot(4 - by)
                ref = detour(slot, n)
                await_bytes(ref, h_recv.at[by - 1, n])
                push(ref, ref, d_send.at[1 + n // 4], d_recv.at[1 + n // 4], sibling)

    for a in range(2):
        relay_x(5, a)

    await_bytes(win_all.at[y], own_sem.at[2])
    await_bytes(wout_all.at[y], own_sem.at[3])
    for n, ref in enumerate(smalls):
        for by in range(1, 4):
            await_bytes(ref.at[plane_slot(4 - by)], small_recv.at[n, by - 1])
    for a in range(2):
        await_bytes(pieces_of(a, 24), d_recv.at[a])
    await_bytes(gates_all.at[pl.ds(0, 3), :, pl.ds(0, 4)], d_recv.at[2])

    def micro(step, token):
        i = step // HALVES
        half = lax.rem(step, HALVES)
        rows = rows_of(half)
        here = act.at[i, rows]
        await_bytes(here, act_recv.at[i, half])

        @pl.when(half == 0)
        def _():
            tails[...] = jnp.zeros_like(tails)
            pasts[...] = jnp.zeros_like(pasts)

        @pl.when((z == 0) & (core == 1) & (step == 0))
        def _():
            pl.semaphore_wait(lag_sem, 1)

        prepare(here, vec_all.at[0], scaled, power)

        def one(s, token):
            layer(here, win_all.at[s], wout_all.at[s], gates_all.at[s], vec_all.at[s],
                  vec_all.at[lax.rem(s + 1, PLANE)], spike_all.at[s, rows], tails.at[s],
                  pasts.at[s], scaled, power, states)

            @pl.when((z == 0) & (core == 0) & (step == 0) & (s == 2))
            def _():
                pl.semaphore_signal(lag_sem, inc=1, device_id=sibling, device_id_type=MESH)

            return token

        lax.fori_loop(0, PLANE, one, 0)

        @pl.when(z < planes - 1)
        def _():
            pltpu.make_async_remote_copy(
                src_ref=here, dst_ref=here, send_sem=act_send.at[i, half],
                recv_sem=act_recv.at[i, half],
                device_id={"pp": lax.rem(z + 1, planes) * PLANE + y}, device_id_type=MESH,
            ).start()

        @pl.when(z == planes - 1)
        def _():
            reorder(here, final.at[i, rows], True)

            @pl.when(i < planes - 1)
            def _():
                pltpu.make_async_remote_copy(
                    src_ref=final.at[i, rows], dst_ref=out.at[0, 0, rows],
                    send_sem=act_send.at[i, half], recv_sem=out_recv.at[half],
                    device_id={"pp": i * PLANE + y}, device_id_type=MESH,
                ).start()

            @pl.when(i == planes - 1)
            def _():
                pltpu.make_async_copy(
                    final.at[i, rows], out.at[0, 0, rows], out_recv.at[half]
                ).start()

        return token

    lax.fori_loop(0, planes * HALVES, micro, 0)

    for half in range(HALVES):
        rows = slice(half * chunk, (half + 1) * chunk)
        await_bytes(out.at[0, 0, rows], out_recv.at[half])
        for i in range(planes):
            if i < planes - 1:
                await_bytes(act.at[i, rows], act_send.at[i, half])
            else:
                @pl.when(z < planes - 1)
                def _():
                    await_bytes(act.at[i, rows], act_send.at[i, half])

        @pl.when(z != 0)
        def _():
            await_bytes(home.at[rows], home_sem.at[half])

    for n, ref in enumerate(smalls):
        for by in range(1, 4):
            await_bytes(ref.at[y], small_send.at[n, by - 1])
    for side in range(2):
        for sem in (y_send, x_send):
            await_bytes(pieces_of(0, 6), sem.at[side, 0])

            @pl.when(first)
            def _():
                await_bytes(wout_all.at[0, pl.ds(0, 9), upper], sem.at[side, 1])

            @pl.when(z != 0)
            def _():
                await_bytes(pieces_of(1, 6), sem.at[side, 1])

        @pl.when(z != 0)
        def _():
            await_bytes(gates_all.at[pl.ds(0, 3), :, pl.ds(0, 2)], g_send.at[side])

    @pl.when(first)
    def _():
        await_bytes(relay_wout, f_send.at[0])
        await_bytes(relay_gate, f_send.at[1])

    @pl.when(last)
    def _():
        await_bytes(onward_wout, k_send.at[0])
        await_bytes(onward_gate, k_send.at[1])
        await_bytes(wout_all.at[0, pl.ds(0, 12), upper], h_send.at[0])
        await_bytes(gates_all.at[pl.ds(0, 3), :, pl.ds(0, 4)], h_send.at[1])

    for a in range(2):
        await_bytes(pieces_of(a, 24), d_send.at[a])
    await_bytes(gates_all.at[pl.ds(0, 3), :, pl.ds(0, 4)], d_send.at[2])


def local(
    tokens,
    layer_norm_scale,
    input_weight,
    filter_weight,
    filter_bias,
    recur_gate_weight,
    recur_gate_bias,
    input_gate_weight,
    input_gate_bias,
    decay_setting,
    spike_log_decay,
    output_weight,
):
    planes = lax.axis_size("pp") // PLANE
    columns = lax.axis_size("fs")
    length, width = tokens.shape[2:]
    inner = input_weight.shape[2]
    blocks = recur_gate_weight.shape[1]
    dma = pltpu.SemaphoreType.DMA
    hbm = pl.BlockSpec(memory_space=pl.ANY)
    near = pl.BlockSpec(memory_space=pltpu.VMEM)
    bf16, f32 = jnp.bfloat16, jnp.float32
    return pl.pallas_call(
        functools.partial(kernel, planes, columns),
        out_shape=jax.ShapeDtypeStruct(tokens.shape, bf16),
        in_specs=[hbm, near, hbm, near, near, hbm, near, hbm, near, near, near, hbm],
        out_specs=near,
        scratch_shapes=[
            pltpu.VMEM((PLANE, inner // 128, width, 128), bf16),
            pltpu.VMEM((PLANE, width // 128, inner, 128), bf16),
            pltpu.VMEM((PLANE, 2, blocks, 128, 128), bf16),
            pltpu.VMEM((PLANE, 16, inner), f32),
            pltpu.VMEM((PLANE, length, 128), f32),
            pltpu.VMEM((length, width), bf16),
            pltpu.VMEM((length, width), bf16),
            pltpu.VMEM((planes, length, width), bf16),
            pltpu.VMEM((planes, length, width), bf16),
            pltpu.VMEM((PLANE, 3 * SUB, inner), f32),
            pltpu.VMEM((PLANE, SUB, inner), f32),
            pltpu.VMEM((length // HALVES, width), bf16),
            pltpu.VMEM((length // HALVES, 128), f32),
            pltpu.VMEM((length // HALVES, inner), bf16),
            pltpu.VMEM((4, inner // 2, 128), bf16),
            pltpu.VMEM((2, 4, 128, 128), bf16),
            pltpu.VMEM((4, inner // 2, 128), bf16),
            pltpu.VMEM((2, 4, 128, 128), bf16),
            dma((2, 6, 2)),
            dma((2, 6, 2)),
            dma((3,)),
            dma((2, 3)),
            dma((2, 2)),
            dma((2, 2)),
            dma((3,)),
            dma((2,)),
            dma((4,)),
            dma((2, 3)),
            dma((2, 3)),
            dma,
            dma((planes, HALVES)),
            dma((planes, HALVES)),
            dma((HALVES,)),
            dma((HALVES,)),
            pltpu.SemaphoreType.REGULAR,
            dma((2,)),
            dma((5,)),
            dma((2,)),
            dma((3, 5)),
            dma((2,)),
            dma((5,)),
        ],
        compiler_params=pltpu.CompilerParams(
            collective_id=0, has_side_effects=True, vmem_limit_bytes=60 * 1024 * 1024
        ),
    )(
        tokens,
        layer_norm_scale,
        input_weight,
        filter_weight,
        filter_bias,
        recur_gate_weight,
        recur_gate_bias,
        input_gate_weight,
        input_gate_bias,
        decay_setting,
        spike_log_decay,
        output_weight,
    )


def solution(mesh):
    placed = (
        P("pp", ("fs", "tp"), None, None),
        P("pp", None),
        P("pp", None, None),
        P("pp", None, None),
        P("pp", None),
        P("pp", None, None, None),
        P("pp", None),
        P("pp", None, None, None),
        P("pp", None),
        P("pp", None),
        P("pp", None),
        P("pp", None, None),
    )
    return jax.shard_map(
        local,
        mesh=mesh,
        in_specs=placed,
        out_specs=P("pp", ("fs", "tp"), None, None),
        check_vma=False,
    )
```
